512 devices in a mesh: sp: 64 (over z, y), tp: 8 (over x, core).
Axes of the slice: x: 4, y: 4, z: 16, core: 2. Of those that a mesh axis runs over, the one named last changes fastest.
Arguments:
- incoming_activity: bfloat16 [32768, 2048], P(('sp', 'tp')), may hold values from -6 to 6
- entry_standardize_factor: bfloat16 [2048], replicated, may hold values from 0.099609375 to 1.8984375
- recursive_entry_matrix: bfloat16 [2048, 2048], P(None, 'tp'), may hold values from -0.125 to 0.125
- final_switch_matrix: bfloat16 [2048, 2048], P(None, 'tp'), may hold values from -0.125 to 0.125
- averaging_entry_matrix: bfloat16 [2048, 1024], P(None, 'tp'), may hold values from -0.125 to 0.125
- percolumn_filter_coefficients: bfloat16 [4, 2048], P(None, 'tp'), may hold values from -3 to 3
- switch_tiled_matrices: bfloat16 [2, 2, 32, 64, 64], P(None, None, 'tp'), may hold values from -0.75 to 0.75
- prior_fading_odds: float32 [2, 2048], P(None, 'tp'), may hold values from 2.7 to 17
- speed_factors: float32 [2, 32768], P(None, 'sp'), may hold values from 0.4 to 2.5, as said below
- extra_fading_amounts: float32 [2, 32768], P(None, 'sp'), may hold values from -1.39 to 0, as said below
- averaging_cluster_matrices: bfloat16 [8, 128, 128], P('tp'), may hold values from -0.5 to 0.5
- averaging_feature_factor: bfloat16 [1024], P('tp'), may hold values from 0.099609375 to 1.8984375
- recursive_final_matrix: bfloat16 [2048, 2048], P('tp'), may hold values from -0.25 to 0.25
- averaging_final_matrix: bfloat16 [1024, 2048], P('tp'), may hold values from -0.1875 to 0.1875
Outputs:
- mixed: bfloat16 [32768, 2048], P(('sp', 'tp'))
The draws below stay inside these ranges and needn't reach their ends.
Inputs may be any that keep to these rules, and one draw needn't show every extreme that they name: `speed_factors`: constant over each aligned block of 512 positions. `extra_fading_amounts`: each row has at most two nonzero entries.
All inputs are finite; a program needn't handle non-finite values.
Results may differ from the reference program's by a relative error of at most 0.017.
Values may be sent and summed in bfloat16 or wider, within the bound.
No kernel may reach another device: no remote copies, remote signals or barrier semaphores. Data moves between devices by JAX's collectives and lax.ppermute only.
A program may use at most 128 MiB of HBM per device.

```python
import jax
import jax.numpy as jnp
from jax import lax

D = 2048
RG_BW = 64
POOL_GROUPS = 8
CONV_W = 4
TOK_SP = 512
D_RNN = 2048
D_POOL = 1024
RG_BLOCKS = 32
POOL_GW = 128
TOKENS = 32768


def draw_prior_fading_odds(key, part):
    pick_key, slow_key, fast_key = jax.random.split(jax.random.fold_in(key, 11), 3)
    share = 0.5
    slow = jax.random.uniform(pick_key, (2, D_RNN), jnp.float32) < share
    slow_rate = jnp.exp(jax.random.uniform(slow_key, (2, D_RNN), jnp.float32, jnp.log(0.004), jnp.log(0.04))) / TOKENS
    fast_rate = jnp.exp(jax.random.uniform(fast_key, (2, D_RNN), jnp.float32, jnp.log(0.02), jnp.log(0.06)))
    fading_speed = jnp.where(slow, slow_rate, fast_rate)
    return -jnp.log(jnp.expm1(fading_speed))


def draw_speed_factors(key, part):
    block_key = jax.random.fold_in(key, 23)
    blocks = TOKENS // TOK_SP
    factor = jnp.exp(jax.random.uniform(block_key, (2, blocks), jnp.float32, jnp.log(0.4), jnp.log(2.5)))
    return jnp.repeat(factor, TOK_SP, axis=1)


def draw_extra_fading_amounts(key, part):
    spot_key, size_key = jax.random.split(jax.random.fold_in(key, 37))
    spots = jax.random.randint(spot_key, (2, 2, 1), 0, TOKENS)
    sizes = jnp.log(jax.random.uniform(size_key, (2, 2, 1), jnp.float32, 0.5, 0.8))
    positions = jnp.arange(TOKENS)[None, None, :]
    return jnp.sum(jnp.where(positions == spots, sizes, 0.0), axis=1)


def level_of(own_key, extent, shards, least, largest):
    loudness = 1.0
    for axis_at, parts in shards:
        heights = jax.random.uniform(jax.random.fold_in(jax.random.fold_in(own_key, 6), axis_at), (parts,), jnp.float32, least / len(shards), largest / len(shards))
        loudness = loudness * jnp.repeat(jnp.exp(heights), extent[axis_at] // parts).reshape((-1,) + (1,) * (len(extent) - 1 - axis_at))
    return loudness


def centred(key, extent, width, most, cuts=(), dtype=jnp.bfloat16):
    array = width * jax.random.normal(key, extent, jnp.float32)
    if cuts:
        array = array * level_of(key, extent, cuts, -0.22, 0.18)
    return jnp.clip(array, -most, most).astype(dtype)


def setup_inputs(seed: int = 0) -> dict:
    arg_keys = jax.random.split(jax.random.key(seed), 15)
    return {
        "incoming_activity": centred(arg_keys[0], (TOKENS, D), 1.0, 6.0, ((0, 512),)),
        "entry_standardize_factor": jnp.clip(1.0 + 0.18 * jax.random.normal(arg_keys[1], (D,), jnp.float32), 0.099609375, 1.8984375).astype(jnp.bfloat16),
        "recursive_entry_matrix": centred(arg_keys[2], (D, D_RNN), D ** -0.5, 0.125, ((1, 8),)),
        "final_switch_matrix": centred(arg_keys[3], (D, D_RNN), D ** -0.5, 0.125, ((1, 8),)),
        "averaging_entry_matrix": centred(arg_keys[4], (D, D_POOL), D ** -0.5, 0.125, ((1, 8),)),
        "percolumn_filter_coefficients": centred(arg_keys[5], (CONV_W, D_RNN), CONV_W ** -0.5, 3.0, ((1, 8),)),
        "switch_tiled_matrices": centred(arg_keys[6], (2, 2, RG_BLOCKS, RG_BW, RG_BW), RG_BW ** -0.5, 0.75, ((2, 8),)),
        "prior_fading_odds": draw_prior_fading_odds(jax.random.fold_in(arg_keys[14], 71), 0),
        "speed_factors": draw_speed_factors(jax.random.fold_in(arg_keys[14], 71), 0),
        "extra_fading_amounts": draw_extra_fading_amounts(jax.random.fold_in(arg_keys[14], 71), 0),
        "averaging_cluster_matrices": centred(arg_keys[10], (POOL_GROUPS, POOL_GW, POOL_GW), POOL_GW ** -0.5, 0.5, ((0, 8),)),
        "averaging_feature_factor": jnp.clip(1.0 + 0.18 * jax.random.normal(arg_keys[11], (D_POOL,), jnp.float32), 0.099609375, 1.8984375).astype(jnp.bfloat16),
        "recursive_final_matrix": centred(arg_keys[12], (D_RNN, D), (D_RNN // 4) ** -0.5, 0.25, ((0, 8),)),
        "averaging_final_matrix": centred(arg_keys[13], (D_POOL, D), D_POOL ** -0.5, 0.1875, ((0, 8),)),
    }


FADING_FACTOR = 8.0
epsilon = 1e-06

def combine(earlier, later):
    return (earlier[0] * later[0], later[0] * earlier[1] + later[1])

def product(left, right):
    return jnp.dot(left, right, preferred_element_type=jnp.float32)

def reference(incoming_activity, entry_standardize_factor, recursive_entry_matrix, final_switch_matrix, averaging_entry_matrix, percolumn_filter_coefficients, switch_tiled_matrices, prior_fading_odds, speed_factors, extra_fading_amounts, averaging_cluster_matrices, averaging_feature_factor, recursive_final_matrix, averaging_final_matrix):
    values = incoming_activity.astype(jnp.float32)
    scaled = values * lax.rsqrt(lax.optimization_barrier(jnp.mean(values * values, axis=1, keepdims=True)) + epsilon)
    normed = (scaled * entry_standardize_factor.astype(jnp.float32)).astype(jnp.bfloat16)
    state_input = product(normed, recursive_entry_matrix).astype(jnp.bfloat16)
    gate_input = product(normed, final_switch_matrix).astype(jnp.bfloat16)
    pool_input = product(normed, averaging_entry_matrix).astype(jnp.bfloat16)
    length = incoming_activity.shape[0]
    padded = jnp.pad(state_input.astype(jnp.float32), ((2, 1), (0, 0)))
    filtered = percolumn_filter_coefficients[0].astype(jnp.float32) * padded[0:length]
    for shift in range(1, CONV_W):
        filtered = filtered + percolumn_filter_coefficients[shift].astype(jnp.float32) * padded[shift:shift + length]
    filtered = filtered.astype(jnp.bfloat16)
    filtered_wide = filtered.astype(jnp.float32)
    blocks = filtered_wide.reshape(length, RG_BLOCKS, RG_BW)
    state_sum = jnp.zeros((length, D_RNN), jnp.float32)
    for sweep_orientation in range(2):
        gate_sums = jnp.einsum('tbi,qbij->tqbj', blocks, switch_tiled_matrices[sweep_orientation].astype(jnp.float32)).reshape(length, 2, D_RNN)
        remember_switch = jax.nn.sigmoid(gate_sums[:, 0])
        inlet = jax.nn.sigmoid(gate_sums[:, 1])
        fading_speed = jax.nn.softplus(-prior_fading_odds[sweep_orientation])
        logarithmic_persistence = -FADING_FACTOR * speed_factors[sweep_orientation][:, None] * remember_switch * fading_speed[None, :] + extra_fading_amounts[sweep_orientation][:, None]
        drive = jnp.sqrt(-jnp.expm1(2.0 * logarithmic_persistence)) * inlet * filtered_wide
        unused, states = lax.associative_scan(combine, (jnp.exp(logarithmic_persistence), drive), axis=0, reverse=sweep_orientation == 1)
        state_sum = state_sum + states
    state_mix = (jax.nn.gelu(gate_input.astype(jnp.float32)) * state_sum).astype(jnp.bfloat16)
    pool_wide = pool_input.astype(jnp.float32)
    pool_padded = jnp.pad(pool_wide, ((8, 8), (0, 0)))
    positions = jnp.arange(length).astype(jnp.int32)
    groups = []
    for group in range(POOL_GROUPS):
        half = 2 ** (group % 4)
        first = group * POOL_GW
        total = jnp.zeros((length, POOL_GW), jnp.float32)
        for offset in range(2 * half):
            begin = 8 - half + offset
            total = total + pool_padded[begin:begin + length, first:first + POOL_GW]
        upper = jnp.minimum(positions + half, length)
        lower = jnp.maximum(positions - half, 0)
        counted = (upper - lower).astype(jnp.float32)[:, None]
        groups.append(total / counted - pool_wide[:, first:first + POOL_GW])
    pooled = jnp.concatenate(groups, axis=1).astype(jnp.bfloat16)
    grouped = jnp.einsum('tgi,gij->tgj', pooled.astype(jnp.float32).reshape(length, POOL_GROUPS, POOL_GW), averaging_cluster_matrices.astype(jnp.float32)).reshape(length, D_POOL)
    pool_mix = (grouped * averaging_feature_factor.astype(jnp.float32)).astype(jnp.bfloat16)
    return (product(state_mix, recursive_final_matrix) + product(pool_mix, averaging_final_matrix)).astype(jnp.bfloat16)
```

```python
import jax
import jax.numpy as jnp
from jax import lax
from jax.experimental import pallas as pl
from jax.experimental.pallas import tpu as pltpu
from jax.sharding import PartitionSpec as P

FADING_FACTOR = 8.0
epsilon = 1e-06

SEG = 8
STEP = 64
ROWS = SEG * STEP
EDGE = 8
WIDE = 2048
CH = 256
PC = 128
F32 = jnp.float32
BF16 = jnp.bfloat16
VMEM = pltpu.VMEM


def vspecs(n):
    return [pl.BlockSpec(memory_space=VMEM)] * n


def params():
    return pltpu.CompilerParams(vmem_limit_bytes=48 * 1024 * 1024)


def cost(flops, nbytes, trans=0):
    return pl.CostEstimate(flops=flops, bytes_accessed=nbytes, transcendentals=trans)


def dot(a, b):
    return jnp.dot(a, b, preferred_element_type=F32)


def normalize(read, write, gain_ref, rows):
    total = jnp.zeros((rows, 128), F32)
    for k in range(WIDE // 128):
        v = read(k * 128).astype(F32)
        total = total + v * v
    inv = lax.rsqrt(jnp.sum(total, axis=1, keepdims=True) * (1.0 / WIDE) + epsilon)
    for k in range(WIDE // 128):
        v = read(k * 128).astype(F32)
        gain = gain_ref[0:1, k * 128 : (k + 1) * 128].astype(F32)
        write(k * 128, ((v * inv) * gain).astype(BF16))


def normalize_shards(x_ref, gain_ref, out_ref):
    def one(i, _):
        base = pl.multiple_of(i * STEP, STEP)

        def read(lane):
            return x_ref[i, :, lane : lane + 128]

        def write(lane, v):
            out_ref[pl.ds(base, STEP), lane : lane + 128] = v

        normalize(read, write, gain_ref, STEP)
        return 0

    lax.fori_loop(0, 4, one, 0)


def project_kernel(x_ref, gain_ref, ws_ref, wg_ref, wp_ref, y_ref, xn_ref):
    normalize_shards(x_ref, gain_ref, xn_ref)
    xn = xn_ref[...]
    y_ref[:, 0:256] = dot(xn, ws_ref[...]).astype(BF16)
    y_ref[:, 256:512] = dot(xn, wg_ref[...]).astype(BF16)
    y_ref[:, 512:640] = dot(xn, wp_ref[...]).astype(BF16)


def gates_kernel(
    x_ref, h1_ref, h2_ref, yo_ref, gain_ref, ws_ref, wg_ref, wp_ref, perm_ref, conv_ref, bd_ref,
    half_rate_ref, extra_ref,
    kd_ref, gate_ref, pool_ref, seg_ref, send_ref,
    xn_ref, y_ref, s_ref, f_ref, g_ref,
):
    normalize_shards(x_ref, gain_ref, xn_ref)
    for n, ref in enumerate((h1_ref, h2_ref)):
        base = 256 + n * EDGE

        def read(lane, ref=ref):
            return ref[:, lane : lane + 128]

        def write(lane, v, base=base):
            xn_ref[base : base + EDGE, lane : lane + 128] = v

        normalize(read, write, gain_ref, EDGE)
    y_ref[0:256, :] = yo_ref[...]
    xn = xn_ref[...]
    y_ref[256:528, 0:256] = dot(xn, ws_ref[...]).astype(BF16)
    y_ref[256:528, 256:512] = dot(xn, wg_ref[...]).astype(BF16)
    y_ref[256:528, 512:640] = dot(xn, wp_ref[...]).astype(BF16)
    lo = (EDGE - 2) * SEG
    s_ref[...] = dot(perm_ref[lo : lo + 67 * SEG, :], y_ref[:, 0:256])
    mid = EDGE * SEG
    gate_ref[...] = dot(perm_ref[mid : mid + ROWS, :], y_ref[:, 256:512])
    pool_ref[...] = dot(perm_ref[...], y_ref[:, 512:640])
    taps = conv_ref[...].astype(F32)

    def conv(i, _):
        base = pl.multiple_of(i * 64, 64)
        value = taps[0:1] * s_ref[pl.ds(base, 64), :]
        for k in range(1, 4):
            value = value + taps[k : k + 1] * s_ref[pl.ds(base + 8 * k, 64), :]
        f_ref[pl.ds(base, 64), :] = value.astype(BF16)
        return 0

    lax.fori_loop(0, ROWS // 64, conv, 0)
    f = f_ref[...]
    for k in range(4):
        g_ref[:, k * 256 : (k + 1) * 256] = dot(f, bd_ref[:, k * 256 : (k + 1) * 256])

    def chunk(i, carry):
        base = pl.multiple_of(i * 64, 64)
        rows = pl.ds(base, 64)
        out = []
        for lt in range(2):
            hf, lf, hb, pb, lb = carry[lt]
            lanes = slice(lt * 128, lt * 128 + 128)
            wide = f_ref[rows, lanes].astype(F32)
            for d in range(2):
                col = d * 512 + lt * 128
                half = half_rate_ref[d : d + 1, lanes]
                recall = jnp.tanh(0.5 * g_ref[rows, col : col + 128])
                inlet = 0.5 * jnp.tanh(0.5 * g_ref[rows, col + 256 : col + 384]) + 0.5
                log_keep = half * recall + half + extra_ref[d, rows, :]
                keep = jnp.exp(log_keep)
                gap = (1.0 + keep * keep) * jnp.tanh(-log_keep)
                drive = gap * lax.rsqrt(jnp.maximum(gap, 1e-37)) * (inlet * wide)
                kd_ref[2 * d, rows, lanes] = keep
                kd_ref[2 * d + 1, rows, lanes] = drive
                for j in range(8):
                    kj = keep[8 * j : 8 * j + 8]
                    uj = drive[8 * j : 8 * j + 8]
                    lj = log_keep[8 * j : 8 * j + 8]
                    if d == 0:
                        hf = kj * hf + uj
                        lf = lf + lj
                    else:
                        hb = hb + pb * uj
                        pb = pb * kj
                        lb = lb + lj
            out.append((hf, lf, hb, pb, lb))
        return tuple(out)

    zero = jnp.zeros((SEG, 128), F32)
    one = jnp.ones((SEG, 128), F32)
    totals = lax.fori_loop(0, ROWS // 64, chunk, tuple((zero, zero, zero, one, zero) for _ in range(2)))
    row = lax.broadcasted_iota(jnp.int32, (SEG, 128), 0)
    send = jnp.zeros((SEG, 128), F32)
    for lt in range(2):
        hf, lf, hb, pb, lb = totals[lt]
        lanes = slice(lt * 128, lt * 128 + 128)
        for d, (log_total, state) in enumerate(((lf, hf), (lb, hb))):
            factor = jnp.exp(log_total)
            for shift in (1, 2, 4):
                move = shift if d == 0 else SEG - shift
                inside = (row >= shift) if d == 0 else (row < SEG - shift)
                earlier_factor = jnp.where(inside, pltpu.roll(factor, move, 0), 1.0)
                earlier_state = jnp.where(inside, pltpu.roll(state, move, 0), 0.0)
                state = factor * earlier_state + state
                factor = factor * earlier_factor
            move = 1 if d == 0 else SEG - 1
            inside = (row >= 1) if d == 0 else (row < SEG - 1)
            seg_ref[2 * d, :, lanes] = jnp.where(inside, pltpu.roll(factor, move, 0), 1.0)
            seg_ref[2 * d + 1, :, lanes] = jnp.where(inside, pltpu.roll(state, move, 0), 0.0)
            end = SEG - 1 if d == 0 else 0
            whole_log = jnp.sum(log_total, axis=0, keepdims=True)
            whole_state = jnp.sum(jnp.where(row == end, state, 0.0), axis=0, keepdims=True)
            send = jnp.where(row == 4 * d + lt, whole_log, send)
            send = jnp.where(row == 4 * d + 2 + lt, whole_state, send)
    packed = send.astype(BF16)
    send_ref[...] = jnp.broadcast_to(packed[None], send_ref.shape)


def pooling_kernel(gate_ref, pool_ref, inverse_ref, code_ref, cluster_ref, factor_ref, act_ref, mix_ref, p_ref):
    def gelu(i, _):
        rows = pl.ds(pl.multiple_of(i * 64, 64), 64)
        v = gate_ref[rows, :]
        inner = 0.7978845608028654 * (v + 0.044715 * (v * v * v))
        act_ref[rows, :] = v * (0.5 * (1.0 + jnp.tanh(inner)))
        return 0

    lax.fori_loop(0, ROWS // 64, gelu, 0)
    code = code_ref[0]

    def windows(i, _):
        base = pl.multiple_of(i * 64, 64)
        level = pool_ref[pl.ds(base, 64 + 2 * EDGE * SEG), :]
        centre = level[EDGE * SEG : EDGE * SEG + 64]
        chosen = jnp.zeros((64, PC), F32)
        for k in range(4):
            shift = SEG << k
            size = level.shape[0] - shift
            level = level[:size] + level[shift:]
            begin = (EDGE - (1 << k)) * SEG
            chosen = jnp.where(code == k, level[begin : begin + 64], chosen)
        rows = pl.ds(base, 64)
        p_ref[rows, :] = (chosen * inverse_ref[rows, :] - centre).astype(BF16)
        return 0

    lax.fori_loop(0, ROWS // 64, windows, 0)
    grouped = dot(p_ref[...], cluster_ref[...])
    mix_ref[...] = (grouped * factor_ref[...].astype(F32)).astype(BF16)


def states_kernel(
    got_ref, after_ref, valid_ref, seg_ref, kd_ref, act_ref, pool_mix_ref, back_ref,
    send_ref, own_ref,
    hf_ref, hb_ref, mix_ref,
):
    got = got_ref[...].reshape(-1, 128)
    sums = dot(after_ref[...], got)
    terms = jnp.exp(sums) * valid_ref[...] * got.astype(F32)
    carry = jnp.sum(terms.reshape(-1, SEG, 128), axis=0)
    begin = []
    for lt in range(2):
        lanes = slice(lt * 128, lt * 128 + 128)
        for d in range(2):
            r = 4 * d + 2 + lt
            begin.append(seg_ref[2 * d, :, lanes] * carry[r : r + 1] + seg_ref[2 * d + 1, :, lanes])

    def walk(i, carry):
        hf0, hb0, hf1, hb1 = carry
        for k in range(8):
            f = pl.ds(pl.multiple_of((i * 8 + k) * SEG, SEG), SEG)
            b = pl.ds(pl.multiple_of((STEP - 1 - i * 8 - k) * SEG, SEG), SEG)
            hf0 = kd_ref[0, f, 0:128] * hf0 + kd_ref[1, f, 0:128]
            hf1 = kd_ref[0, f, 128:256] * hf1 + kd_ref[1, f, 128:256]
            hb0 = kd_ref[2, b, 0:128] * hb0 + kd_ref[3, b, 0:128]
            hb1 = kd_ref[2, b, 128:256] * hb1 + kd_ref[3, b, 128:256]
            hf_ref[f, 0:128] = hf0
            hf_ref[f, 128:256] = hf1
            hb_ref[b, 0:128] = hb0
            hb_ref[b, 128:256] = hb1
        return hf0, hb0, hf1, hb1

    lax.fori_loop(0, STEP // 8, walk, tuple(begin))

    def mixing(i, _):
        rows = pl.ds(pl.multiple_of(i * 64, 64), 64)
        mix_ref[rows, 0:CH] = (act_ref[rows, :] * (hf_ref[rows, :] + hb_ref[rows, :])).astype(BF16)
        return 0

    lax.fori_loop(0, ROWS // 64, mixing, 0)
    mix_ref[:, CH : CH + PC] = pool_mix_ref[...]
    mix = mix_ref[...]
    send_ref[...] = dot(back_ref[0:256, :], mix).astype(BF16)
    own_ref[...] = dot(back_ref[256:512, :], mix).astype(BF16)


def output_kernel(own_ref, got_ref, wr_ref, wp_ref, vr_ref, vp_ref, out_ref):
    own_state = own_ref[:, 0:CH]
    own_pool = own_ref[:, CH : CH + PC]
    got_state = got_ref[:, 0:CH]
    got_pool = got_ref[:, CH : CH + PC]
    for k in range(4):
        lanes = slice(k * 512, k * 512 + 512)
        value = dot(own_state, wr_ref[:, lanes]) + dot(got_state, vr_ref[:, lanes])
        value = value + dot(own_pool, wp_ref[:, lanes]) + dot(got_pool, vp_ref[:, lanes])
        value = value.astype(BF16)
        for x in range(4):
            out_ref[x, :, lanes] = value[x * STEP : (x + 1) * STEP]


def local(
    incoming_activity,
    entry_standardize_factor,
    recursive_entry_matrix,
    final_switch_matrix,
    averaging_entry_matrix,
    percolumn_filter_coefficients,
    switch_tiled_matrices,
    prior_fading_odds,
    speed_factors,
    extra_fading_amounts,
    averaging_cluster_matrices,
    averaging_feature_factor,
    recursive_final_matrix,
    averaging_final_matrix,
):
    blocks = lax.axis_size("sp")
    place = lax.axis_index("sp")
    column = lax.axis_index("tp")
    core = column % 2
    same_core = [[0, 2, 4, 6], [1, 3, 5, 7]]
    sibling = [(k, k ^ 1) for k in range(8)]

    def exchange(v):
        return lax.all_to_all(
            v, "tp", split_axis=0, concat_axis=0, tiled=True, axis_index_groups=same_core
        )

    def edge_pairs(cross):
        pairs = []
        for sp in range(blocks):
            for tp in range(8):
                to = sp + 1 if tp % 2 else sp - 1
                if 0 <= to < blocks:
                    pairs.append((sp * 8 + tp, to * 8 + (tp ^ cross)))
        return pairs

    x_own = exchange(jnp.broadcast_to(incoming_activity, (4, *incoming_activity.shape)))
    edge = lax.dynamic_slice(
        x_own, (3 * core, (STEP - EDGE) * core, 0), (1, EDGE, WIDE)
    ).reshape(EDGE, WIDE)
    edge_same = lax.ppermute(edge, ("sp", "tp"), edge_pairs(0))
    edge_cross = lax.ppermute(edge, ("sp", "tp"), edge_pairs(1))
    x_sibling = lax.ppermute(x_own, "tp", sibling)
    sibling_recursive = lax.ppermute(recursive_final_matrix, "tp", sibling)
    sibling_averaging = lax.ppermute(averaging_final_matrix, "tp", sibling)

    wide_row = jnp.arange((STEP + 2 * EDGE) * SEG, dtype=jnp.int32)
    t = (wide_row % SEG) * STEP + wide_row // SEG - EDGE
    shard = t // STEP
    held = jnp.where(shard % 2 == core, 0, 256) + (shard // 2) * STEP + t % STEP
    before = jnp.where(core == 1, 512, 520)
    held = jnp.where(t < 0, before + t + EDGE, held)
    held = jnp.where(t >= ROWS, (1032 - before) + t - ROWS, held)
    perm = (held[:, None] == jnp.arange(528, dtype=jnp.int32)[None, :]).astype(BF16)
    out_row = jnp.arange(ROWS, dtype=jnp.int32)
    parity = jnp.where(out_row < 256, 1 - core, core)
    source = (out_row % STEP) * SEG + 2 * ((out_row % 256) // STEP) + parity
    back = (source[:, None] == jnp.arange(ROWS, dtype=jnp.int32)[None, :]).astype(BF16)

    entry = jnp.arange(blocks * SEG, dtype=jnp.int32)
    p, r = entry[:, None] // SEG, entry[:, None] % SEG
    q, r2 = entry[None, :] // SEG, entry[None, :] % SEG
    between = jnp.where(r < 4, (q > p) & (q < place), (q < p) & (q > place))
    after = (between & (r2 == r - 2) & (r % 4 >= 2)).astype(BF16)
    valid = jnp.where(r < 4, p < place, p > place) & (r % 4 >= 2)
    valid = jnp.broadcast_to(valid.astype(F32), (blocks * SEG, 128))

    eye = jnp.eye(4, dtype=BF16)
    maps = jnp.transpose(switch_tiled_matrices, (2, 3, 0, 1, 4))
    maps = (maps[:, :, :, :, None, :] * eye[:, None, None, None, :, None]).reshape(CH, 4 * CH)
    half_rate = (-0.5 * FADING_FACTOR) * speed_factors[:, :1] * jax.nn.softplus(-prior_fading_odds)
    extra = jnp.transpose(extra_fading_amounts.reshape(2, SEG, STEP), (0, 2, 1)).reshape(2, ROWS, 1)
    extra = jnp.broadcast_to(extra, (2, ROWS, 128))
    window_code = column % 4
    reach = jnp.left_shift(1, window_code)
    mid_row = jnp.arange(ROWS, dtype=jnp.int32)
    position = place * ROWS + (mid_row % SEG) * STEP + mid_row // SEG
    count = jnp.minimum(position + reach, ROWS * blocks) - jnp.maximum(position - reach, 0)
    inverse = jnp.broadcast_to((1.0 / count.astype(F32))[:, None], (ROWS, PC))
    gain = entry_standardize_factor.reshape(1, WIDE)
    entry_weights = (recursive_entry_matrix, final_switch_matrix, averaging_entry_matrix)

    y_own = pl.pallas_call(
        project_kernel,
        out_shape=jax.ShapeDtypeStruct((256, 640), BF16),
        in_specs=vspecs(5),
        out_specs=pl.BlockSpec(memory_space=VMEM),
        scratch_shapes=[VMEM((256, WIDE), BF16)],
        compiler_params=params(),
        cost_estimate=cost(2 * 256 * WIDE * 640, 4_000_000),
        name="project",
    )(x_own, gain, *entry_weights)

    kd, gate, pool, seg, send = pl.pallas_call(
        gates_kernel,
        out_shape=(
            jax.ShapeDtypeStruct((4, ROWS, CH), F32),
            jax.ShapeDtypeStruct((ROWS, CH), F32),
            jax.ShapeDtypeStruct((ROWS + 2 * EDGE * SEG, PC), F32),
            jax.ShapeDtypeStruct((4, SEG, CH), F32),
            jax.ShapeDtypeStruct((blocks, SEG, 128), BF16),
        ),
        in_specs=vspecs(13),
        out_specs=tuple(vspecs(5)),
        scratch_shapes=[
            VMEM((272, WIDE), BF16),
            VMEM((528, 640), BF16),
            VMEM((67 * SEG, CH), F32),
            VMEM((ROWS, CH), BF16),
            VMEM((ROWS, 4 * CH), F32),
        ],
        compiler_params=params(),
        cost_estimate=cost(4 * 272 * WIDE * 640, 8_000_000, 1_000_000),
        name="gates",
    )(
        x_sibling, edge_same, edge_cross, y_own, gain, *entry_weights, perm,
        percolumn_filter_coefficients, maps, half_rate, extra,
    )

    got = lax.all_to_all(send, "sp", split_axis=0, concat_axis=0, tiled=True)

    act, pool_mix = pl.pallas_call(
        pooling_kernel,
        out_shape=(
            jax.ShapeDtypeStruct((ROWS, CH), F32),
            jax.ShapeDtypeStruct((ROWS, PC), BF16),
        ),
        in_specs=[*vspecs(3), pl.BlockSpec(memory_space=pltpu.SMEM), *vspecs(2)],
        out_specs=tuple(vspecs(2)),
        scratch_shapes=[VMEM((ROWS, PC), BF16)],
        compiler_params=params(),
        cost_estimate=cost(1_000_000_000, 2_000_000, 200_000),
        name="pooling",
    )(
        gate, pool, inverse, window_code.reshape(1), averaging_cluster_matrices.reshape(PC, PC),
        averaging_feature_factor.reshape(1, PC),
    )

    mix_send, mix_own = pl.pallas_call(
        states_kernel,
        out_shape=(
            jax.ShapeDtypeStruct((256, CH + PC), BF16),
            jax.ShapeDtypeStruct((256, CH + PC), BF16),
        ),
        in_specs=vspecs(8),
        out_specs=tuple(vspecs(2)),
        scratch_shapes=[
            VMEM((ROWS, CH), F32),
            VMEM((ROWS, CH), F32),
            VMEM((ROWS, CH + PC), BF16),
        ],
        compiler_params=params(),
        cost_estimate=cost(1_000_000_000, 4_000_000, 100_000),
        name="states",
    )(got, after, valid, seg, kd, act, pool_mix, back)

    mix_got = lax.ppermute(mix_send, "tp", sibling)

    partial = pl.pallas_call(
        output_kernel,
        out_shape=jax.ShapeDtypeStruct((4, STEP, WIDE), BF16),
        in_specs=vspecs(6),
        out_specs=pl.BlockSpec(memory_space=VMEM),
        compiler_params=params(),
        cost_estimate=cost(4 * 256 * 384 * WIDE, 5_000_000),
        name="output",
    )(
        mix_own, mix_got, recursive_final_matrix, averaging_final_matrix, sibling_recursive,
        sibling_averaging,
    )
    moved = exchange(partial)
    return jnp.sum(moved.astype(F32), axis=0).astype(BF16)


def solution(mesh):
    in_specs = (
        P(("sp", "tp"), None),
        P(),
        P(None, "tp"),
        P(None, "tp"),
        P(None, "tp"),
        P(None, "tp"),
        P(None, None, "tp", None, None),
        P(None, "tp"),
        P(None, "sp"),
        P(None, "sp"),
        P("tp", None, None),
        P("tp"),
        P("tp", None),
        P("tp", None),
    )
    out_specs = P(("sp", "tp"), None)
    return jax.shard_map(local, mesh=mesh, in_specs=in_specs, out_specs=out_specs, check_vma=False)
```

```python
import jax
import jax.numpy as jnp
from jax import lax
from jax.experimental import pallas as pl
from jax.experimental.pallas import tpu as pltpu
from jax.sharding import PartitionSpec as P

FADING_FACTOR = 8.0
epsilon = 1e-06

SEG = 8
STEP = 64
ROWS = SEG * STEP
EDGE = 8
WIDE = 2048
CH = 256
PC = 128
F32 = jnp.float32
BF16 = jnp.bfloat16
VMEM = pltpu.VMEM
HBM = pltpu.HBM
DMA = pltpu.SemaphoreType.DMA
PITCH = STEP + 3 * EDGE


def vspecs(n):
    return [pl.BlockSpec(memory_space=VMEM)] * n


def hspecs(n):
    return [pl.BlockSpec(memory_space=HBM)] * n


def kept(*arrays):
    return [pltpu.with_memory_space_constraint(array, HBM) for array in arrays]


def params(mebibytes):
    return pltpu.CompilerParams(vmem_limit_bytes=mebibytes * 1024 * 1024)


def cost(flops, nbytes, trans=0):
    return pl.CostEstimate(flops=flops, bytes_accessed=nbytes, transcendentals=trans)


def dot(a, b):
    return jnp.dot(a, b, preferred_element_type=F32)


def normalize(read, write, gain_ref, rows):
    total = jnp.zeros((rows, 128), F32)
    for k in range(WIDE // 128):
        v = read(k * 128).astype(F32)
        total = total + v * v
    inv = lax.rsqrt(jnp.sum(total, axis=1, keepdims=True) * (1.0 / WIDE) + epsilon)
    for k in range(WIDE // 128):
        v = read(k * 128).astype(F32)
        gain = gain_ref[0:1, k * 128 : (k + 1) * 128].astype(F32)
        write(k * 128, ((v * inv) * gain).astype(BF16))


def normalize_shards(x_ref, gain_ref, out_ref):
    def one(i, _):
        base = pl.multiple_of(i * STEP, STEP)

        def read(lane):
            return x_ref[i, :, lane : lane + 128]

        def write(lane, v):
            out_ref[pl.ds(base, STEP), lane : lane + 128] = v

        normalize(read, write, gain_ref, STEP)
        return 0

    lax.fori_loop(0, 4, one, 0)


def spread_kernel(x_ref, out_ref, held_ref, in_sem, out_sem):
    load = pltpu.make_async_copy(x_ref, held_ref, in_sem)
    load.start()
    load.wait()
    copies = [pltpu.make_async_copy(held_ref, out_ref.at[k], out_sem.at[k]) for k in range(4)]
    for copy in copies:
        copy.start()
    for copy in copies:
        copy.wait()


def tables_kernel(maps_ref, extra_ref, bd_ref, spread_ref):
    bd_ref[...] = jnp.zeros_like(bd_ref)
    blank = jnp.zeros((64, 64), BF16)
    for d in range(2):
        for q in range(2):
            for b in range(4):
                block = maps_ref[d, q, b]
                tile = jnp.concatenate([block, blank] if b % 2 == 0 else [blank, block], axis=1)
                col = (d * 2 + q) * CH + (b // 2) * 128
                bd_ref[b * 64 : b * 64 + 64, col : col + 128] = tile
    for d in range(2):
        for j in range(STEP):
            spread_ref[d, j * SEG : (j + 1) * SEG, :] = jnp.broadcast_to(
                extra_ref[d, :, j : j + 1], (SEG, 128)
            )


def project_kernel(x_ref, gain_ref, ws_ref, wg_ref, wp_ref, y_ref, xn_ref):
    normalize_shards(x_ref, gain_ref, xn_ref)
    xn = xn_ref[...]
    y_ref[:, 0:256] = dot(xn, ws_ref[...]).astype(BF16)
    y_ref[:, 256:512] = dot(xn, wg_ref[...]).astype(BF16)
    y_ref[:, 512:640] = dot(xn, wp_ref[...]).astype(BF16)


def gates_kernel(
    at_ref, x_ref, h1_ref, h2_ref, yo_ref, gain_ref, ws_ref, wg_ref, wp_ref, conv_ref, bd_ref,
    half_rate_ref, extra_ref,
    kd_out, gate_out, pool_out, seg_out, send_ref,
    x_held, xn_ref, y_ref, f_ref, g_ref, kd_ref, gate_ref, pool_ref, seg_ref,
    x_sem, kd_sem, gate_sem, pool_sem, seg_sem,
):
    core = lax.rem(at_ref[1], 2)
    loads = [pltpu.make_async_copy(x_ref.at[x], x_held.at[x], x_sem.at[x]) for x in range(4)]
    for load in loads:
        load.start()
    for x in range(4):
        base = pl.multiple_of((2 * x + core) * PITCH + EDGE, 8)
        for k in range(5):
            tile = yo_ref[x * STEP : (x + 1) * STEP, k * 128 : (k + 1) * 128]
            y_ref[k, pl.ds(base, STEP), :] = tile.astype(F32)
    for n, ref in enumerate((h1_ref, h2_ref)):
        base = 256 + n * EDGE

        def read_edge(lane, ref=ref):
            return ref[:, lane : lane + 128]

        def write_edge(lane, v, base=base):
            xn_ref[base : base + EDGE, lane : lane + 128] = v

        normalize(read_edge, write_edge, gain_ref, EDGE)
    for x in range(4):
        loads[x].wait()

        def read(lane, x=x):
            return x_held[x, :, lane : lane + 128]

        def write(lane, v, x=x):
            xn_ref[x * STEP : (x + 1) * STEP, lane : lane + 128] = v

        normalize(read, write, gain_ref, STEP)
    xn = xn_ref[...]
    first = 0
    for w_ref in (ws_ref, wg_ref, wp_ref):
        value = dot(xn, w_ref[...]).astype(BF16).astype(F32)
        for n in range(w_ref.shape[1] // 128):
            k = first + n
            tile = value[:, n * 128 : (n + 1) * 128]
            for x in range(4):
                base = pl.multiple_of((2 * x + 1 - core) * PITCH + EDGE, 8)
                y_ref[k, pl.ds(base, STEP), :] = tile[x * STEP : (x + 1) * STEP]
            if k in (0, 1, 4):
                one, two = tile[256 : 256 + EDGE], tile[256 + EDGE : 256 + 2 * EDGE]
                y_ref[k, 0:EDGE, :] = jnp.where(core == 1, one, two)
                end = (SEG - 1) * PITCH + EDGE + STEP
                y_ref[k, end : end + EDGE, :] = jnp.where(core == 1, two, one)
                for s in range(SEG - 1):
                    low, high = s * PITCH, (s + 1) * PITCH
                    y_ref[k, high : high + EDGE, :] = y_ref[k, low + STEP : low + STEP + EDGE, :]
                    y_ref[k, low + EDGE + STEP : low + 2 * EDGE + STEP, :] = y_ref[
                        k, high + EDGE : high + 2 * EDGE, :
                    ]
        first += w_ref.shape[1] // 128

    def at(k, j):
        return y_ref[k, pl.ds(j + EDGE, SEG, stride=PITCH), :]

    taps = conv_ref[...].astype(F32)

    def conv(i, _):
        rows = pl.ds(pl.multiple_of(i * 64, 64), 64)
        for lt in range(2):
            lanes = slice(lt * 128, lt * 128 + 128)
            near = [at(lt, i * 8 + j - 2) for j in range(11)]
            out = []
            for j in range(8):
                value = taps[0:1, lanes] * near[j]
                for k in range(1, 4):
                    value = value + taps[k : k + 1, lanes] * near[j + k]
                out.append(value)
            f_ref[rows, lanes] = jnp.concatenate(out, axis=0).astype(BF16)
            gate = [at(2 + lt, i * 8 + j) for j in range(8)]
            gate_ref[rows, lanes] = jnp.concatenate(gate, axis=0).astype(BF16)
        return 0

    lax.fori_loop(0, STEP // 8, conv, 0)
    gate_copy = pltpu.make_async_copy(gate_ref, gate_out, gate_sem)
    gate_copy.start()

    def pools(i, _):
        rows = pl.ds(pl.multiple_of(i * 64, 64), 64)
        tiles = [at(4, i * 8 + j - EDGE) for j in range(8)]
        pool_ref[rows, :] = jnp.concatenate(tiles, axis=0).astype(BF16)
        return 0

    lax.fori_loop(0, (STEP + 2 * EDGE) // 8, pools, 0)
    pool_copy = pltpu.make_async_copy(pool_ref, pool_out, pool_sem)
    pool_copy.start()
    f = f_ref[...]
    for k in range(4):
        g_ref[:, k * 256 : (k + 1) * 256] = dot(f, bd_ref[:, k * 256 : (k + 1) * 256])

    def chunk(i, carry):
        rows = pl.ds(pl.multiple_of(i * 64, 64), 64)
        out = []
        for lt in range(2):
            hf, lf, hb, pb, lb = carry[lt]
            lanes = slice(lt * 128, lt * 128 + 128)
            wide = f_ref[rows, lanes].astype(F32)
            for d in range(2):
                col = d * 512 + lt * 128
                half = half_rate_ref[d : d + 1, lanes]
                recall = jnp.tanh(0.5 * g_ref[rows, col : col + 128])
                inlet = 0.5 * jnp.tanh(0.5 * g_ref[rows, col + 256 : col + 384]) + 0.5
                log_keep = half * recall + half + extra_ref[d, rows, :]
                keep = jnp.exp(log_keep)
                gap = (1.0 + keep * keep) * jnp.tanh(-log_keep)
                drive = gap * lax.rsqrt(jnp.maximum(gap, 1e-37)) * (inlet * wide)
                kd_ref[2 * d, rows, lanes] = keep
                kd_ref[2 * d + 1, rows, lanes] = drive
                for j in range(8):
                    kj = keep[8 * j : 8 * j + 8]
                    uj = drive[8 * j : 8 * j + 8]
                    lj = log_keep[8 * j : 8 * j + 8]
                    if d == 0:
                        hf = kj * hf + uj
                        lf = lf + lj
                    else:
                        hb = hb + pb * uj
                        pb = pb * kj
                        lb = lb + lj
            out.append((hf, lf, hb, pb, lb))
        return tuple(out)

    zero = jnp.zeros((SEG, 128), F32)
    one = jnp.ones((SEG, 128), F32)
    totals = tuple((zero, zero, zero, one, zero) for _ in range(2))
    kd_copies = []
    for part in range(4):
        totals = lax.fori_loop(2 * part, 2 * part + 2, chunk, totals)
        rows = slice(part * 128, part * 128 + 128)
        copy = pltpu.make_async_copy(
            kd_ref.at[:, rows, :], kd_out.at[:, rows, :], kd_sem.at[part]
        )
        copy.start()
        kd_copies.append(copy)
    row = lax.broadcasted_iota(jnp.int32, (SEG, 128), 0)
    send = jnp.zeros((SEG, 128), F32)
    for lt in range(2):
        hf, lf, hb, _, lb = totals[lt]
        lanes = slice(lt * 128, lt * 128 + 128)
        for d, (log_total, state) in enumerate(((lf, hf), (lb, hb))):
            factor = jnp.exp(log_total)
            for shift in (1, 2, 4):
                move = shift if d == 0 else SEG - shift
                inside = (row >= shift) if d == 0 else (row < SEG - shift)
                earlier_factor = jnp.where(inside, pltpu.roll(factor, move, 0), 1.0)
                earlier_state = jnp.where(inside, pltpu.roll(state, move, 0), 0.0)
                state = factor * earlier_state + state
                factor = factor * earlier_factor
            move = 1 if d == 0 else SEG - 1
            inside = (row >= 1) if d == 0 else (row < SEG - 1)
            seg_ref[2 * d, :, lanes] = jnp.where(inside, pltpu.roll(factor, move, 0), 1.0)
            seg_ref[2 * d + 1, :, lanes] = jnp.where(inside, pltpu.roll(state, move, 0), 0.0)
            end = SEG - 1 if d == 0 else 0
            whole_log = jnp.sum(log_total, axis=0, keepdims=True)
            whole_state = jnp.sum(jnp.where(row == end, state, 0.0), axis=0, keepdims=True)
            send = jnp.where(row == 4 * d + lt, whole_log, send)
            send = jnp.where(row == 4 * d + 2 + lt, whole_state, send)
    seg_copy = pltpu.make_async_copy(seg_ref, seg_out, seg_sem)
    seg_copy.start()
    packed = send.astype(BF16)
    send_ref[...] = jnp.broadcast_to(packed[None], send_ref.shape)
    for copy in (gate_copy, pool_copy, seg_copy, *kd_copies):
        copy.wait()


def pooling_kernel(at_ref, pool_ref, cluster_ref, factor_ref, mix_ref, p_ref):
    place, column = at_ref[0], at_ref[1]
    total = at_ref[2]
    code = lax.rem(column, 4)

    def windows(i, _):
        base = pl.multiple_of(i * 64, 64)
        level = pool_ref[pl.ds(base, 64 + 2 * EDGE * SEG), :].astype(F32)
        centre = level[EDGE * SEG : EDGE * SEG + 64]
        chosen = jnp.zeros((64, PC), F32)
        for k in range(4):
            shift = SEG << k
            size = level.shape[0] - shift
            level = level[:size] + level[shift:]
            begin = (EDGE - (1 << k)) * SEG
            chosen = jnp.where(code == k, level[begin : begin + 64], chosen)
        row = base + lax.broadcasted_iota(jnp.int32, (64, PC), 0)
        position = place * ROWS + (row & 7) * STEP + (row >> 3)
        reach = jnp.left_shift(1, code)
        count = jnp.minimum(position + reach, total) - jnp.maximum(position - reach, 0)
        p_ref[pl.ds(base, 64), :] = (chosen / count.astype(F32) - centre).astype(BF16)
        return 0

    lax.fori_loop(0, ROWS // 64, windows, 0)
    grouped = dot(p_ref[...], cluster_ref[...])
    mix_ref[...] = (grouped * factor_ref[...].astype(F32)).astype(BF16)


def states_kernel(
    at_ref, got_ref, seg_ref, kd_ref, gate_ref, pool_mix_ref,
    send_ref, own_ref,
    hf_ref, hb_ref, mix_ref,
):
    place = at_ref[0]
    core = lax.rem(at_ref[1], 2)
    blocks = got_ref.shape[0]

    def arriving(i, carry):
        ahead, behind = carry
        for k in range(2):
            p = i * 2 + k
            v = got_ref[p].astype(F32)
            ahead = jnp.where(p < place, jnp.exp(pltpu.roll(v, 2, 0)) * ahead + v, ahead)
            p = blocks - 1 - p
            v = got_ref[p].astype(F32)
            behind = jnp.where(p > place, jnp.exp(pltpu.roll(v, 2, 0)) * behind + v, behind)
        return ahead, behind

    zero = jnp.zeros((SEG, 128), F32)
    carry = lax.fori_loop(0, blocks // 2, arriving, (zero, zero), unroll=min(8, blocks // 2))
    begin = []
    for lt in range(2):
        lanes = slice(lt * 128, lt * 128 + 128)
        for d in range(2):
            r = 4 * d + 2 + lt
            begin.append(
                seg_ref[2 * d, :, lanes] * carry[d][r : r + 1] + seg_ref[2 * d + 1, :, lanes]
            )

    def walk(i, carry):
        hf0, hb0, hf1, hb1 = carry
        for k in range(8):
            f = pl.ds(pl.multiple_of((i * 8 + k) * SEG, SEG), SEG)
            b = pl.ds(pl.multiple_of((STEP - 1 - i * 8 - k) * SEG, SEG), SEG)
            hf0 = kd_ref[0, f, 0:128] * hf0 + kd_ref[1, f, 0:128]
            hf1 = kd_ref[0, f, 128:256] * hf1 + kd_ref[1, f, 128:256]
            hb0 = kd_ref[2, b, 0:128] * hb0 + kd_ref[3, b, 0:128]
            hb1 = kd_ref[2, b, 128:256] * hb1 + kd_ref[3, b, 128:256]
            hf_ref[f, 0:128] = hf0
            hf_ref[f, 128:256] = hf1
            hb_ref[b, 0:128] = hb0
            hb_ref[b, 128:256] = hb1
        return hf0, hb0, hf1, hb1

    lax.fori_loop(0, STEP // 8, walk, tuple(begin))

    def mixing(i, _):
        rows = pl.ds(pl.multiple_of(i * 64, 64), 64)
        for lt in range(2):
            lanes = slice(lt * 128, lt * 128 + 128)
            v = gate_ref[rows, lanes].astype(F32)
            inner = 0.7978845608028654 * (v + 0.044715 * (v * v * v))
            act = v * (0.5 * (1.0 + jnp.tanh(inner)))
            mix_ref[lt, rows, :] = act * (hf_ref[rows, lanes] + hb_ref[rows, lanes])
        mix_ref[2, rows, :] = pool_mix_ref[rows, :].astype(F32)
        return 0

    lax.fori_loop(0, ROWS // 64, mixing, 0)
    for x in range(4):
        rows = slice(x * STEP, (x + 1) * STEP)
        for k in range(3):
            lanes = slice(k * 128, k * 128 + 128)
            there = mix_ref[k, pl.ds(2 * x + 1 - core, STEP, stride=SEG), :]
            send_ref[rows, lanes] = there.astype(BF16)
            here = mix_ref[k, pl.ds(2 * x + core, STEP, stride=SEG), :]
            own_ref[rows, lanes] = here.astype(BF16)


def output_kernel(
    own_ref, got_ref, wr_hbm, wp_hbm, vr_hbm, vp_hbm, out_ref, wr_ref, wp_ref, vr_ref, vp_ref, sem
):
    pairs = ((wr_hbm, wr_ref), (wp_hbm, wp_ref), (vr_hbm, vr_ref), (vp_hbm, vp_ref))
    copies = []
    for k in range(4):
        lanes = slice(k * 512, k * 512 + 512)
        copies.append(
            [
                pltpu.make_async_copy(source.at[:, lanes], target.at[:, lanes], sem.at[k, n])
                for n, (source, target) in enumerate(pairs)
            ]
        )
        for copy in copies[k]:
            copy.start()
    own_state = own_ref[:, 0:CH]
    own_pool = own_ref[:, CH : CH + PC]
    got_state = got_ref[:, 0:CH]
    got_pool = got_ref[:, CH : CH + PC]
    for k in range(4):
        lanes = slice(k * 512, k * 512 + 512)
        for copy in copies[k]:
            copy.wait()
        value = dot(own_state, wr_ref[:, lanes]) + dot(got_state, vr_ref[:, lanes])
        value = value + dot(own_pool, wp_ref[:, lanes]) + dot(got_pool, vp_ref[:, lanes])
        value = value.astype(BF16)
        for x in range(4):
            out_ref[x, :, lanes] = value[x * STEP : (x + 1) * STEP]


def local(
    incoming_activity,
    entry_standardize_factor,
    recursive_entry_matrix,
    final_switch_matrix,
    averaging_entry_matrix,
    percolumn_filter_coefficients,
    switch_tiled_matrices,
    prior_fading_odds,
    speed_factors,
    extra_fading_amounts,
    averaging_cluster_matrices,
    averaging_feature_factor,
    recursive_final_matrix,
    averaging_final_matrix,
):
    blocks = lax.axis_size("sp")
    place = lax.axis_index("sp")
    column = lax.axis_index("tp")
    core = column % 2
    same_core = [[0, 2, 4, 6], [1, 3, 5, 7]]
    sibling = [(k, k ^ 1) for k in range(8)]

    def exchange(v):
        return lax.all_to_all(
            v, "tp", split_axis=0, concat_axis=0, tiled=True, axis_index_groups=same_core
        )

    def edge_pairs(cross):
        pairs = []
        for sp in range(blocks):
            for tp in range(8):
                to = sp + 1 if tp % 2 else sp - 1
                if 0 <= to < blocks:
                    pairs.append((sp * 8 + tp, to * 8 + (tp ^ cross)))
        return pairs

    spread = pl.pallas_call(
        spread_kernel,
        out_shape=HBM((4, STEP, WIDE), BF16),
        in_specs=hspecs(1),
        out_specs=pl.BlockSpec(memory_space=HBM),
        scratch_shapes=[VMEM((STEP, WIDE), BF16), DMA, DMA((4,))],
        compiler_params=params(2),
        cost_estimate=cost(0, 1_300_000),
        name="spread",
    )(*kept(incoming_activity))
    spread, *later = lax.optimization_barrier(
        (spread, switch_tiled_matrices, recursive_final_matrix, averaging_final_matrix)
    )
    x_own = exchange(spread)
    at = jnp.stack([place, column, jnp.asarray(blocks * ROWS)]).astype(jnp.int32)
    half_rate = (-0.5 * FADING_FACTOR) * speed_factors[:, :1] * jax.nn.softplus(-prior_fading_odds)
    gain = entry_standardize_factor.reshape(1, WIDE)
    smem = pl.BlockSpec(memory_space=pltpu.SMEM)
    maps, extra = pl.pallas_call(
        tables_kernel,
        out_shape=(
            HBM((CH, 4 * CH), BF16),
            HBM((2, ROWS, 128), F32),
        ),
        in_specs=vspecs(2),
        out_specs=tuple(vspecs(2)),
        compiler_params=params(4),
        cost_estimate=cost(1_000_000, 2_000_000),
        name="tables",
    )(later[0], extra_fading_amounts.reshape(2, SEG, STEP))
    sibling_recursive = lax.ppermute(later[1], "tp", sibling)
    sibling_averaging = lax.ppermute(later[2], "tp", sibling)
    x_own, maps, extra, half_rate, gain, at, sibling_recursive, sibling_averaging = (
        lax.optimization_barrier(
            (x_own, maps, extra, half_rate, gain, at, sibling_recursive, sibling_averaging)
        )
    )
    edge = lax.dynamic_slice(
        x_own, (3 * core, (STEP - EDGE) * core, 0), (1, EDGE, WIDE)
    ).reshape(EDGE, WIDE)
    edge_same = lax.ppermute(edge, ("sp", "tp"), edge_pairs(0))
    edge_cross = lax.ppermute(edge, ("sp", "tp"), edge_pairs(1))
    x_sibling = lax.ppermute(x_own, "tp", sibling)
    entry_weights = (recursive_entry_matrix, final_switch_matrix, averaging_entry_matrix)

    y_own = pl.pallas_call(
        project_kernel,
        out_shape=jax.ShapeDtypeStruct((256, 640), BF16),
        in_specs=vspecs(5),
        out_specs=pl.BlockSpec(memory_space=VMEM),
        scratch_shapes=[VMEM((256, WIDE), BF16)],
        compiler_params=params(8),
        cost_estimate=cost(2 * 256 * WIDE * 640, 4_000_000),
        name="project",
    )(x_own, gain, *entry_weights)

    kd, gate, pool, seg, send = pl.pallas_call(
        gates_kernel,
        out_shape=(
            HBM((4, ROWS, CH), F32),
            HBM((ROWS, CH), BF16),
            HBM((ROWS + 2 * EDGE * SEG, PC), BF16),
            HBM((4, SEG, CH), F32),
            jax.ShapeDtypeStruct((blocks, SEG, 128), BF16),
        ),
        in_specs=[smem, *hspecs(1), *vspecs(11)],
        out_specs=(*hspecs(4), *vspecs(1)),
        scratch_shapes=[
            VMEM((4, STEP, WIDE), BF16),
            VMEM((272, WIDE), BF16),
            VMEM((5, SEG * PITCH, 128), F32),
            VMEM((ROWS, CH), BF16),
            VMEM((ROWS, 4 * CH), F32),
            VMEM((4, ROWS, CH), F32),
            VMEM((ROWS, CH), BF16),
            VMEM((ROWS + 2 * EDGE * SEG, PC), BF16),
            VMEM((4, SEG, CH), F32),
            DMA((4,)),
            DMA((4,)),
            DMA,
            DMA,
            DMA,
        ],
        compiler_params=params(20),
        cost_estimate=cost(4 * 272 * WIDE * 640, 8_000_000, 1_000_000),
        name="gates",
    )(
        at, *kept(x_sibling), edge_same, edge_cross, y_own, gain, *entry_weights,
        percolumn_filter_coefficients, maps, half_rate, extra,
    )

    got = lax.all_to_all(send, "sp", split_axis=0, concat_axis=0, tiled=True)

    pool_mix = pl.pallas_call(
        pooling_kernel,
        out_shape=jax.ShapeDtypeStruct((ROWS, PC), BF16),
        in_specs=[smem, *vspecs(3)],
        out_specs=pl.BlockSpec(memory_space=VMEM),
        scratch_shapes=[VMEM((ROWS, PC), BF16)],
        compiler_params=params(4),
        cost_estimate=cost(1_000_000_000, 2_000_000, 200_000),
        name="pooling",
    )(
        at, pool, averaging_cluster_matrices.reshape(PC, PC),
        averaging_feature_factor.reshape(1, PC),
    )

    mix_send, mix_own = pl.pallas_call(
        states_kernel,
        out_shape=(
            jax.ShapeDtypeStruct((256, CH + PC), BF16),
            jax.ShapeDtypeStruct((256, CH + PC), BF16),
        ),
        in_specs=[smem, *vspecs(5)],
        out_specs=tuple(vspecs(2)),
        scratch_shapes=[
            VMEM((ROWS, CH), F32),
            VMEM((ROWS, CH), F32),
            VMEM((3, ROWS, 128), F32),
        ],
        compiler_params=params(8),
        cost_estimate=cost(1_000_000_000, 4_000_000, 100_000),
        name="states",
    )(at, got, seg, kd, gate, pool_mix)

    mix_got = lax.ppermute(mix_send, "tp", sibling)

    partial = pl.pallas_call(
        output_kernel,
        out_shape=jax.ShapeDtypeStruct((4, STEP, WIDE), BF16),
        in_specs=[*vspecs(2), *hspecs(4)],
        out_specs=pl.BlockSpec(memory_space=VMEM),
        scratch_shapes=[
            VMEM((CH, WIDE), BF16),
            VMEM((PC, WIDE), BF16),
            VMEM((CH, WIDE), BF16),
            VMEM((PC, WIDE), BF16),
            DMA((4, 4)),
        ],
        compiler_params=params(10),
        cost_estimate=cost(4 * 256 * 384 * WIDE, 5_000_000),
        name="output",
    )(
        mix_own,
        mix_got,
        *kept(recursive_final_matrix, averaging_final_matrix, sibling_recursive, sibling_averaging),
    )
    moved = exchange(partial)
    return jnp.sum(moved.astype(F32), axis=0).astype(BF16)


def solution(mesh):
    in_specs = (
        P(("sp", "tp"), None),
        P(),
        P(None, "tp"),
        P(None, "tp"),
        P(None, "tp"),
        P(None, "tp"),
        P(None, None, "tp", None, None),
        P(None, "tp"),
        P(None, "sp"),
        P(None, "sp"),
        P("tp", None, None),
        P("tp"),
        P("tp", None),
        P("tp", None),
    )
    out_specs = P(("sp", "tp"), None)


    return jax.shard_map(local, mesh=mesh, in_specs=in_specs, out_specs=out_specs, check_vma=False)
```

```python
import jax
import jax.numpy as jnp
from jax import lax
from jax.experimental import pallas as pl
from jax.experimental.pallas import tpu as pltpu
from jax.sharding import PartitionSpec as P

FADING_FACTOR = 8.0
epsilon = 1e-06

SEG = 8
STEP = 64
ROWS = SEG * STEP
EDGE = 8
WIDE = 2048
CH = 256
PC = 128
F32 = jnp.float32
BF16 = jnp.bfloat16
VMEM = pltpu.VMEM
HBM = pltpu.HBM
DMA = pltpu.SemaphoreType.DMA
PITCH = STEP + 3 * EDGE


def vspecs(n):
    return [pl.BlockSpec(memory_space=VMEM)] * n


def hspecs(n):
    return [pl.BlockSpec(memory_space=HBM)] * n


def kept(*arrays):
    return [pltpu.with_memory_space_constraint(array, HBM) for array in arrays]


def params(mebibytes):
    return pltpu.CompilerParams(vmem_limit_bytes=mebibytes * 1024 * 1024)


def cost(flops, nbytes, trans=0):
    return pl.CostEstimate(flops=flops, bytes_accessed=nbytes, transcendentals=trans)


def dot(a, b):
    return jnp.dot(a, b, preferred_element_type=F32)


def normalize(read, write, gain_ref, rows):
    total = jnp.zeros((rows, 128), F32)
    for k in range(WIDE // 128):
        v = read(k * 128).astype(F32)
        total = total + v * v
    inv = lax.rsqrt(jnp.sum(total, axis=1, keepdims=True) * (1.0 / WIDE) + epsilon)
    for k in range(WIDE // 128):
        v = read(k * 128).astype(F32)
        gain = gain_ref[0:1, k * 128 : (k + 1) * 128].astype(F32)
        write(k * 128, ((v * inv) * gain).astype(BF16))


def normalize_shard(x_ref, gain_ref, out_ref, base):
    def read(lane):
        return x_ref[:, lane : lane + 128]

    def write(lane, v):
        out_ref[base : base + x_ref.shape[0], lane : lane + 128] = v

    normalize(read, write, gain_ref, x_ref.shape[0])


def tables_kernel(maps_ref, extra_ref, bd_ref, spread_ref):
    bd_ref[...] = jnp.zeros_like(bd_ref)
    blank = jnp.zeros((64, 64), BF16)
    for d in range(2):
        for q in range(2):
            for b in range(4):
                block = maps_ref[d, q, b]
                tile = jnp.concatenate([block, blank] if b % 2 == 0 else [blank, block], axis=1)
                col = (d * 2 + q) * CH + (b // 2) * 128
                bd_ref[b * 64 : b * 64 + 64, col : col + 128] = tile
    for d in range(2):
        for j in range(STEP):
            spread_ref[d, j * SEG : (j + 1) * SEG, :] = jnp.broadcast_to(
                extra_ref[d, :, j : j + 1], (SEG, 128)
            )


def placing(at_ref):
    core = lax.rem(at_ref[1], 2)
    chip = lax.div(at_ref[1], 2)

    def place(y_ref, k, tile, edges):
        for n in range(8):
            parity = core if n < 4 else 1 - core
            segment = 2 * lax.rem(chip + (0, 3, 1, 2)[n % 4], 4) + parity
            rows = pl.ds(pl.multiple_of(segment * PITCH + EDGE, 8), STEP)
            y_ref[k, rows, :] = tile[n * STEP : (n + 1) * STEP]
        if edges:
            one, two = tile[ROWS : ROWS + EDGE], tile[ROWS + EDGE : ROWS + 2 * EDGE]
            y_ref[k, 0:EDGE, :] = jnp.where(core == 1, one, two)
            end = (SEG - 1) * PITCH + EDGE + STEP
            y_ref[k, end : end + EDGE, :] = jnp.where(core == 1, two, one)
            for s in range(SEG - 1):
                low, high = s * PITCH, (s + 1) * PITCH
                y_ref[k, high : high + EDGE, :] = y_ref[k, low + STEP : low + STEP + EDGE, :]
                y_ref[k, low + EDGE + STEP : low + 2 * EDGE + STEP, :] = y_ref[
                    k, high + EDGE : high + 2 * EDGE, :
                ]

    def take(y_ref, k, j):
        return y_ref[k, pl.ds(j + EDGE, SEG, stride=PITCH), :]

    return place, take


def gates_kernel(
    at_ref, x_hbm, xb_ref, xc_ref, xd_ref, sa_ref, sb_ref, sc_ref, sd_ref, h1_ref, h2_ref, gain_ref,
    rate_ref, ws_hbm, conv_hbm, bd_hbm, speed_hbm, extra_hbm,
    kd_out, xn_out, seg_out, send_out,
    x_ref, ws_ref, conv_ref, bd_ref, speed_ref, extra_ref,
    xn_ref, y_ref, f_ref, g_ref, kd_ref, seg_ref, send_ref,
    x_sem, ws_sem, table_sem, kd_sem, xn_sem, seg_sem, send_sem,
):
    place, take = placing(at_ref)
    x_load = pltpu.make_async_copy(x_hbm, x_ref, x_sem)
    x_load.start()
    ws_load = pltpu.make_async_copy(ws_hbm, ws_ref, ws_sem)
    ws_load.start()
    tables = ((conv_hbm, conv_ref), (bd_hbm, bd_ref), (speed_hbm, speed_ref), (extra_hbm, extra_ref))
    table_loads = [
        pltpu.make_async_copy(source, target, table_sem.at[n])
        for n, (source, target) in enumerate(tables)
    ]
    for load in table_loads:
        load.start()
    shards = (xb_ref, xc_ref, xd_ref, sa_ref, sb_ref, sc_ref, sd_ref)
    for n, ref in enumerate(shards):
        normalize_shard(ref, gain_ref, xn_ref, (n + 1) * STEP)
    for n, ref in enumerate((h1_ref, h2_ref)):
        normalize_shard(ref, gain_ref, xn_ref, ROWS + n * EDGE)
    x_load.wait()
    normalize_shard(x_ref, gain_ref, xn_ref, 0)
    xn_copy = pltpu.make_async_copy(xn_ref, xn_out, xn_sem)
    xn_copy.start()
    ws_load.wait()
    value = dot(xn_ref[...], ws_ref[...]).astype(BF16).astype(F32)
    for k in range(2):
        place(y_ref, k, value[:, k * 128 : (k + 1) * 128], True)
    for load in table_loads:
        load.wait()
    taps = conv_ref[...].astype(F32)

    def conv(i, _):
        rows = pl.ds(pl.multiple_of(i * 64, 64), 64)
        for lt in range(2):
            lanes = slice(lt * 128, lt * 128 + 128)
            near = [take(y_ref, lt, i * 8 + j - 2) for j in range(11)]
            out = []
            for j in range(8):
                value = taps[0:1, lanes] * near[j]
                for k in range(1, 4):
                    value = value + taps[k : k + 1, lanes] * near[j + k]
                out.append(value)
            f_ref[rows, lanes] = jnp.concatenate(out, axis=0).astype(BF16)
        return 0

    lax.fori_loop(0, STEP // 8, conv, 0)
    f = f_ref[...]
    for k in range(4):
        g_ref[:, k * 256 : (k + 1) * 256] = dot(f, bd_ref[:, k * 256 : (k + 1) * 256])

    def chunk(i, carry):
        rows = pl.ds(pl.multiple_of(i * 64, 64), 64)
        out = []
        for lt in range(2):
            hf, lf, hb, pb, lb = carry[lt]
            lanes = slice(lt * 128, lt * 128 + 128)
            wide = f_ref[rows, lanes].astype(F32)
            for d in range(2):
                col = d * 512 + lt * 128
                half = half_rate[d][:, lanes]
                recall = jnp.tanh(0.5 * g_ref[rows, col : col + 128])
                inlet = 0.5 * jnp.tanh(0.5 * g_ref[rows, col + 256 : col + 384]) + 0.5
                log_keep = half * recall + half + extra_ref[d, rows, :]
                keep = jnp.exp(log_keep)
                gap = (1.0 + keep * keep) * jnp.tanh(-log_keep)
                drive = gap * lax.rsqrt(jnp.maximum(gap, 1e-37)) * (inlet * wide)
                kd_ref[2 * d, rows, lanes] = keep
                kd_ref[2 * d + 1, rows, lanes] = drive
                for j in range(8):
                    kj = keep[8 * j : 8 * j + 8]
                    uj = drive[8 * j : 8 * j + 8]
                    lj = log_keep[8 * j : 8 * j + 8]
                    if d == 0:
                        hf = kj * hf + uj
                        lf = lf + lj
                    else:
                        hb = hb + pb * uj
                        pb = pb * kj
                        lb = lb + lj
            out.append((hf, lf, hb, pb, lb))
        return tuple(out)

    half_rate = [
        (-0.5 * FADING_FACTOR) * speed_ref[d : d + 1, 0:1] * rate_ref[d : d + 1, :] for d in range(2)
    ]
    zero = jnp.zeros((SEG, 128), F32)
    one = jnp.ones((SEG, 128), F32)
    totals = tuple((zero, zero, zero, one, zero) for _ in range(2))
    kd_copies = []
    for part in range(4):
        totals = lax.fori_loop(2 * part, 2 * part + 2, chunk, totals)
        rows = slice(part * 128, part * 128 + 128)
        copy = pltpu.make_async_copy(
            kd_ref.at[:, rows, :], kd_out.at[:, rows, :], kd_sem.at[part]
        )
        copy.start()
        kd_copies.append(copy)
    row = lax.broadcasted_iota(jnp.int32, (SEG, 128), 0)
    send = jnp.zeros((SEG, 128), F32)
    for lt in range(2):
        hf, lf, hb, _, lb = totals[lt]
        lanes = slice(lt * 128, lt * 128 + 128)
        for d, (log_total, state) in enumerate(((lf, hf), (lb, hb))):
            factor = jnp.exp(log_total)
            for shift in (1, 2, 4):
                move = shift if d == 0 else SEG - shift
                inside = (row >= shift) if d == 0 else (row < SEG - shift)
                earlier_factor = jnp.where(inside, pltpu.roll(factor, move, 0), 1.0)
                earlier_state = jnp.where(inside, pltpu.roll(state, move, 0), 0.0)
                state = factor * earlier_state + state
                factor = factor * earlier_factor
            move = 1 if d == 0 else SEG - 1
            inside = (row >= 1) if d == 0 else (row < SEG - 1)
            seg_ref[2 * d, :, lanes] = jnp.where(inside, pltpu.roll(factor, move, 0), 1.0)
            seg_ref[2 * d + 1, :, lanes] = jnp.where(inside, pltpu.roll(state, move, 0), 0.0)
            end = SEG - 1 if d == 0 else 0
            whole_log = jnp.sum(log_total, axis=0, keepdims=True)
            whole_state = jnp.sum(jnp.where(row == end, state, 0.0), axis=0, keepdims=True)
            send = jnp.where(row == 4 * d + lt, whole_log, send)
            send = jnp.where(row == 4 * d + 2 + lt, whole_state, send)
    seg_copy = pltpu.make_async_copy(seg_ref, seg_out, seg_sem)
    seg_copy.start()
    packed = send.astype(BF16)
    send_ref[...] = jnp.broadcast_to(packed[None], send_ref.shape)
    send_copy = pltpu.make_async_copy(send_ref, send_out, send_sem)
    send_copy.start()
    for copy in (xn_copy, seg_copy, *kd_copies, send_copy):
        copy.wait()


def pooling_kernel(
    at_ref, xn_hbm, wg_hbm, wp_hbm, cluster_ref, factor_ref,
    gate_ref, mix_ref,
    xn_ref, wg_ref, wp_ref, y_ref, pool_ref, p_ref, sem,
):
    loads = [
        pltpu.make_async_copy(source, target, sem.at[n])
        for n, (source, target) in enumerate(((xn_hbm, xn_ref), (wp_hbm, wp_ref), (wg_hbm, wg_ref)))
    ]
    for load in loads:
        load.start()
    place, take = placing(at_ref)
    position_of, column = at_ref[0], at_ref[1]
    total = at_ref[2]
    code = lax.rem(column, 4)
    loads[0].wait()
    loads[1].wait()
    xn = xn_ref[...]
    place(y_ref, 2, dot(xn, wp_ref[...]).astype(BF16).astype(F32), True)
    loads[2].wait()
    value = dot(xn, wg_ref[...]).astype(BF16).astype(F32)
    for k in range(2):
        place(y_ref, k, value[:, k * 128 : (k + 1) * 128], False)

    def gates(i, _):
        rows = pl.ds(pl.multiple_of(i * 64, 64), 64)
        for lt in range(2):
            tiles = [take(y_ref, lt, i * 8 + j) for j in range(8)]
            gate_ref[rows, lt * 128 : lt * 128 + 128] = jnp.concatenate(tiles, axis=0).astype(BF16)
        return 0

    lax.fori_loop(0, STEP // 8, gates, 0)

    def pools(i, _):
        rows = pl.ds(pl.multiple_of(i * 64, 64), 64)
        tiles = [take(y_ref, 2, i * 8 + j - EDGE) for j in range(8)]
        pool_ref[rows, :] = jnp.concatenate(tiles, axis=0)
        return 0

    lax.fori_loop(0, (STEP + 2 * EDGE) // 8, pools, 0)

    def windows(i, _):
        base = pl.multiple_of(i * 64, 64)
        level = pool_ref[pl.ds(base, 64 + 2 * EDGE * SEG), :]
        centre = level[EDGE * SEG : EDGE * SEG + 64]
        chosen = jnp.zeros((64, PC), F32)
        for k in range(4):
            shift = SEG << k
            size = level.shape[0] - shift
            level = level[:size] + level[shift:]
            begin = (EDGE - (1 << k)) * SEG
            chosen = jnp.where(code == k, level[begin : begin + 64], chosen)
        row = base + lax.broadcasted_iota(jnp.int32, (64, PC), 0)
        position = position_of * ROWS + (row & 7) * STEP + (row >> 3)
        reach = jnp.left_shift(1, code)
        count = jnp.minimum(position + reach, total) - jnp.maximum(position - reach, 0)
        p_ref[pl.ds(base, 64), :] = (chosen / count.astype(F32) - centre).astype(BF16)
        return 0

    lax.fori_loop(0, ROWS // 64, windows, 0)
    grouped = dot(p_ref[...], cluster_ref[...])
    mix_ref[...] = (grouped * factor_ref[...].astype(F32)).astype(BF16)


def states_kernel(
    at_ref, got_ref, seg_ref, kd_ref, gate_ref, pool_mix_ref,
    send_ref, own_ref,
    hf_ref, hb_ref, mix_ref,
):
    place = at_ref[0]
    core = lax.rem(at_ref[1], 2)
    blocks = got_ref.shape[0]

    def arriving(i, carry):
        ahead, behind = carry
        for k in range(2):
            p = i * 2 + k
            v = got_ref[p].astype(F32)
            ahead = jnp.where(p < place, jnp.exp(pltpu.roll(v, 2, 0)) * ahead + v, ahead)
            p = blocks - 1 - p
            v = got_ref[p].astype(F32)
            behind = jnp.where(p > place, jnp.exp(pltpu.roll(v, 2, 0)) * behind + v, behind)
        return ahead, behind

    zero = jnp.zeros((SEG, 128), F32)
    carry = lax.fori_loop(0, blocks // 2, arriving, (zero, zero), unroll=min(8, blocks // 2))
    begin = []
    for lt in range(2):
        lanes = slice(lt * 128, lt * 128 + 128)
        for d in range(2):
            r = 4 * d + 2 + lt
            begin.append(
                seg_ref[2 * d, :, lanes] * carry[d][r : r + 1] + seg_ref[2 * d + 1, :, lanes]
            )

    def walk(i, carry):
        hf0, hb0, hf1, hb1 = carry
        for k in range(8):
            f = pl.ds(pl.multiple_of((i * 8 + k) * SEG, SEG), SEG)
            b = pl.ds(pl.multiple_of((STEP - 1 - i * 8 - k) * SEG, SEG), SEG)
            hf0 = kd_ref[0, f, 0:128] * hf0 + kd_ref[1, f, 0:128]
            hf1 = kd_ref[0, f, 128:256] * hf1 + kd_ref[1, f, 128:256]
            hb0 = kd_ref[2, b, 0:128] * hb0 + kd_ref[3, b, 0:128]
            hb1 = kd_ref[2, b, 128:256] * hb1 + kd_ref[3, b, 128:256]
            hf_ref[f, 0:128] = hf0
            hf_ref[f, 128:256] = hf1
            hb_ref[b, 0:128] = hb0
            hb_ref[b, 128:256] = hb1
        return hf0, hb0, hf1, hb1

    lax.fori_loop(0, STEP // 8, walk, tuple(begin))

    def mixing(i, _):
        rows = pl.ds(pl.multiple_of(i * 64, 64), 64)
        for lt in range(2):
            lanes = slice(lt * 128, lt * 128 + 128)
            v = gate_ref[rows, lanes].astype(F32)
            inner = 0.7978845608028654 * (v + 0.044715 * (v * v * v))
            act = v * (0.5 * (1.0 + jnp.tanh(inner)))
            mix_ref[lt, rows, :] = act * (hf_ref[rows, lanes] + hb_ref[rows, lanes])
        mix_ref[2, rows, :] = pool_mix_ref[rows, :].astype(F32)
        return 0

    lax.fori_loop(0, ROWS // 64, mixing, 0)
    for x in range(4):
        rows = slice(x * STEP, (x + 1) * STEP)
        for k in range(3):
            lanes = slice(k * 128, k * 128 + 128)
            there = mix_ref[k, pl.ds(2 * x + 1 - core, STEP, stride=SEG), :]
            send_ref[rows, lanes] = there.astype(BF16)
            here = mix_ref[k, pl.ds(2 * x + core, STEP, stride=SEG), :]
            own_ref[rows, lanes] = here.astype(BF16)


def output_kernel(
    own_ref, got_ref, wr_hbm, wp_hbm, vr_hbm, vp_hbm, out_ref, wr_ref, wp_ref, vr_ref, vp_ref, sem
):
    pairs = ((wr_hbm, wr_ref), (wp_hbm, wp_ref), (vr_hbm, vr_ref), (vp_hbm, vp_ref))
    copies = []
    for k in range(4):
        lanes = slice(k * 512, k * 512 + 512)
        copies.append(
            [
                pltpu.make_async_copy(source.at[:, lanes], target.at[:, lanes], sem.at[k, n])
                for n, (source, target) in enumerate(pairs)
            ]
        )
        for copy in copies[k]:
            copy.start()
    own_state = own_ref[:, 0:CH]
    own_pool = own_ref[:, CH : CH + PC]
    got_state = got_ref[:, 0:CH]
    got_pool = got_ref[:, CH : CH + PC]
    for k in range(4):
        lanes = slice(k * 512, k * 512 + 512)
        for copy in copies[k]:
            copy.wait()
        value = dot(own_state, wr_ref[:, lanes]) + dot(got_state, vr_ref[:, lanes])
        value = value + dot(own_pool, wp_ref[:, lanes]) + dot(got_pool, vp_ref[:, lanes])
        value = value.astype(BF16)
        for x in range(4):
            out_ref[x, :, lanes] = value[x * STEP : (x + 1) * STEP]


def local(
    incoming_activity,
    entry_standardize_factor,
    recursive_entry_matrix,
    final_switch_matrix,
    averaging_entry_matrix,
    percolumn_filter_coefficients,
    switch_tiled_matrices,
    prior_fading_odds,
    speed_factors,
    extra_fading_amounts,
    averaging_cluster_matrices,
    averaging_feature_factor,
    recursive_final_matrix,
    averaging_final_matrix,
):
    blocks = lax.axis_size("sp")
    place = lax.axis_index("sp")
    column = lax.axis_index("tp")
    core = column % 2
    same_core = [[0, 2, 4, 6], [1, 3, 5, 7]]
    sibling = [(k, k ^ 1) for k in range(8)]

    def exchange(v):
        return lax.all_to_all(
            v, "tp", split_axis=0, concat_axis=0, tiled=True, axis_index_groups=same_core
        )

    def edge_pairs(cross):
        pairs = []
        for sp in range(blocks):
            for tp in range(8):
                to = sp + 1 if tp % 2 else sp - 1
                if 0 <= to < blocks:
                    pairs.append((sp * 8 + tp, to * 8 + (tp ^ cross)))
        return pairs

    def to_chip(v, offset):
        return lax.ppermute(v, "tp", [(k, (k + 2 * offset) % 8) for k in range(8)])

    def to_sibling(v):
        return lax.ppermute(v, "tp", sibling)

    x = incoming_activity
    edge_row = (STEP - EDGE) * core
    x_before = to_chip(x, 1)
    x_after = to_chip(x, 3)
    edge_own = lax.dynamic_slice(x, (edge_row, 0), (EDGE, WIDE))
    edge_far = to_chip(edge_own, 2)
    x_far = to_chip(x, 2)
    x_sibling = [to_sibling(x)]
    chip = column // 2
    holder = jnp.where(core == 1, 3 - chip, (4 - chip) % 4)
    edge = jnp.where(holder == 0, edge_own, edge_far)
    edge = jnp.where(holder == 3, lax.dynamic_slice(x_before, (edge_row, 0), (EDGE, WIDE)), edge)
    edge = jnp.where(holder == 1, lax.dynamic_slice(x_after, (edge_row, 0), (EDGE, WIDE)), edge)
    edge_same = lax.ppermute(edge, ("sp", "tp"), edge_pairs(0))
    edge_cross = lax.ppermute(edge, ("sp", "tp"), edge_pairs(1))
    x_sibling.append(to_sibling(x_before))
    x_sibling.append(to_sibling(x_after))
    x_sibling.append(to_sibling(x_far))

    at = jnp.stack([place, column, jnp.asarray(blocks * ROWS)]).astype(jnp.int32)
    gain = entry_standardize_factor.reshape(1, WIDE)
    rate = jax.nn.softplus(-prior_fading_odds)
    smem = pl.BlockSpec(memory_space=pltpu.SMEM)
    maps, extra = pl.pallas_call(
        tables_kernel,
        out_shape=(
            HBM((CH, 4 * CH), BF16),
            HBM((2, ROWS, 128), F32),
        ),
        in_specs=vspecs(2),
        out_specs=tuple(vspecs(2)),
        compiler_params=params(4),
        cost_estimate=cost(1_000_000, 2_000_000),
        name="tables",
    )(switch_tiled_matrices, extra_fading_amounts.reshape(2, SEG, STEP))

    kd, xn, seg, send = pl.pallas_call(
        gates_kernel,
        out_shape=(
            HBM((4, ROWS, CH), F32),
            HBM((ROWS + 2 * EDGE, WIDE), BF16),
            HBM((4, SEG, CH), F32),
            HBM((blocks, SEG, 128), BF16),
        ),
        in_specs=[smem, *hspecs(1), *vspecs(11), *hspecs(5)],
        out_specs=tuple(hspecs(4)),
        scratch_shapes=[
            VMEM((STEP, WIDE), BF16),
            VMEM((WIDE, CH), BF16),
            VMEM((4, CH), BF16),
            VMEM((CH, 4 * CH), BF16),
            VMEM((2, ROWS), F32),
            VMEM((2, ROWS, 128), F32),
            VMEM((ROWS + 2 * EDGE, WIDE), BF16),
            VMEM((2, SEG * PITCH, 128), F32),
            VMEM((ROWS, CH), BF16),
            VMEM((ROWS, 4 * CH), F32),
            VMEM((4, ROWS, CH), F32),
            VMEM((4, SEG, CH), F32),
            VMEM((blocks, SEG, 128), BF16),
            DMA,
            DMA,
            DMA((4,)),
            DMA((4,)),
            DMA,
            DMA,
            DMA,
        ],
        compiler_params=params(20),
        cost_estimate=cost(2 * 528 * WIDE * 256, 8_000_000, 1_000_000),
        name="gates",
    )(
        at, *kept(x), x_before, x_after, x_far, *x_sibling, edge_same, edge_cross, gain, rate,
        *kept(recursive_entry_matrix, percolumn_filter_coefficients, maps, speed_factors, extra),
    )

    send, *later = lax.optimization_barrier((send, recursive_final_matrix, averaging_final_matrix))
    got = lax.all_to_all(send, "sp", split_axis=0, concat_axis=0, tiled=True)
    sibling_recursive = lax.ppermute(later[0], "tp", sibling)
    sibling_averaging = lax.ppermute(later[1], "tp", sibling)

    gate, pool_mix = pl.pallas_call(
        pooling_kernel,
        out_shape=(
            jax.ShapeDtypeStruct((ROWS, CH), BF16),
            jax.ShapeDtypeStruct((ROWS, PC), BF16),
        ),
        in_specs=[smem, *hspecs(3), *vspecs(2)],
        out_specs=tuple(vspecs(2)),
        scratch_shapes=[
            VMEM((ROWS + 2 * EDGE, WIDE), BF16),
            VMEM((WIDE, CH), BF16),
            VMEM((WIDE, PC), BF16),
            VMEM((3, SEG * PITCH, 128), F32),
            VMEM((ROWS + 2 * EDGE * SEG, PC), F32),
            VMEM((ROWS, PC), BF16),
            DMA((3,)),
        ],
        compiler_params=params(16),
        cost_estimate=cost(2 * 528 * WIDE * 384, 6_000_000, 200_000),
        name="pooling",
    )(
        at, *kept(xn, final_switch_matrix, averaging_entry_matrix),
        averaging_cluster_matrices.reshape(PC, PC), averaging_feature_factor.reshape(1, PC),
    )

    mix_send, mix_own = pl.pallas_call(
        states_kernel,
        out_shape=(
            jax.ShapeDtypeStruct((256, CH + PC), BF16),
            jax.ShapeDtypeStruct((256, CH + PC), BF16),
        ),
        in_specs=[smem, *vspecs(5)],
        out_specs=tuple(vspecs(2)),
        scratch_shapes=[
            VMEM((ROWS, CH), F32),
            VMEM((ROWS, CH), F32),
            VMEM((3, ROWS, 128), F32),
        ],
        compiler_params=params(8),
        cost_estimate=cost(1_000_000_000, 4_000_000, 100_000),
        name="states",
    )(at, got, seg, kd, gate, pool_mix)

    mix_got = lax.ppermute(mix_send, "tp", sibling)

    partial = pl.pallas_call(
        output_kernel,
        out_shape=jax.ShapeDtypeStruct((4, STEP, WIDE), BF16),
        in_specs=[*vspecs(2), *hspecs(4)],
        out_specs=pl.BlockSpec(memory_space=VMEM),
        scratch_shapes=[
            VMEM((CH, WIDE), BF16),
            VMEM((PC, WIDE), BF16),
            VMEM((CH, WIDE), BF16),
            VMEM((PC, WIDE), BF16),
            DMA((4, 4)),
        ],
        compiler_params=params(10),
        cost_estimate=cost(4 * 256 * 384 * WIDE, 5_000_000),
        name="output",
    )(
        mix_own,
        mix_got,
        *kept(recursive_final_matrix, averaging_final_matrix, sibling_recursive, sibling_averaging),
    )
    moved = exchange(partial)
    return jnp.sum(moved.astype(F32), axis=0).astype(BF16)


def solution(mesh):
    in_specs = (
        P(("sp", "tp"), None),
        P(),
        P(None, "tp"),
        P(None, "tp"),
        P(None, "tp"),
        P(None, "tp"),
        P(None, None, "tp", None, None),
        P(None, "tp"),
        P(None, "sp"),
        P(None, "sp"),
        P("tp", None, None),
        P("tp"),
        P("tp", None),
        P("tp", None),
    )
    out_specs = P(("sp", "tp"), None)


    return jax.shard_map(local, mesh=mesh, in_specs=in_specs, out_specs=out_specs, check_vma=False)
```

```python
import jax
import jax.numpy as jnp
from jax import lax
from jax.experimental import pallas as pl
from jax.experimental.pallas import tpu as pltpu
from jax.sharding import PartitionSpec as P

FADING_FACTOR = 8.0
epsilon = 1e-06

SEG = 8
STEP = 64
ROWS = SEG * STEP
EDGE = 8
WIDE = 2048
CH = 256
PC = 128
F32 = jnp.float32
BF16 = jnp.bfloat16
VMEM = pltpu.VMEM
HBM = pltpu.HBM
DMA = pltpu.SemaphoreType.DMA
PITCH = STEP + 3 * EDGE


def vspecs(n):
    return [pl.BlockSpec(memory_space=VMEM)] * n


def hspecs(n):
    return [pl.BlockSpec(memory_space=HBM)] * n


def kept(*arrays):
    return [pltpu.with_memory_space_constraint(array, HBM) for array in arrays]


def params(mebibytes):
    return pltpu.CompilerParams(vmem_limit_bytes=mebibytes * 1024 * 1024)


def cost(flops, nbytes, trans=0):
    return pl.CostEstimate(flops=flops, bytes_accessed=nbytes, transcendentals=trans)


def dot(a, b):
    return jnp.dot(a, b, preferred_element_type=F32)


def normalize(read, write, gain_ref, rows):
    total = jnp.zeros((rows, 128), F32)
    for k in range(WIDE // 128):
        v = read(k * 128).astype(F32)
        total = total + v * v
    inv = lax.rsqrt(jnp.sum(total, axis=1, keepdims=True) * (1.0 / WIDE) + epsilon)
    for k in range(WIDE // 128):
        v = read(k * 128).astype(F32)
        gain = gain_ref[0:1, k * 128 : (k + 1) * 128].astype(F32)
        write(k * 128, ((v * inv) * gain).astype(BF16))


def normalize_shard(x_ref, gain_ref, out_ref, base):
    def read(lane):
        return x_ref[:, lane : lane + 128]

    def write(lane, v):
        out_ref[base : base + x_ref.shape[0], lane : lane + 128] = v

    normalize(read, write, gain_ref, x_ref.shape[0])


def spread_kernel(x_ref, out_ref, held_ref, in_sem, out_sem):
    load = pltpu.make_async_copy(x_ref, held_ref, in_sem)
    load.start()
    load.wait()
    copies = [pltpu.make_async_copy(held_ref, out_ref.at[k], out_sem.at[k]) for k in range(4)]
    for copy in copies:
        copy.start()
    for copy in copies:
        copy.wait()


def tables_kernel(maps_ref, extra_ref, bd_ref, spread_ref):
    bd_ref[...] = jnp.zeros_like(bd_ref)
    blank = jnp.zeros((64, 64), BF16)
    for d in range(2):
        for q in range(2):
            for b in range(4):
                block = maps_ref[d, q, b]
                tile = jnp.concatenate([block, blank] if b % 2 == 0 else [blank, block], axis=1)
                col = (d * 2 + q) * CH + (b // 2) * 128
                bd_ref[b * 64 : b * 64 + 64, col : col + 128] = tile
    for d in range(2):
        for j in range(STEP):
            spread_ref[d, j * SEG : (j + 1) * SEG, :] = jnp.broadcast_to(
                extra_ref[d, :, j : j + 1], (SEG, 128)
            )


def placing(at_ref):
    core = lax.rem(at_ref[1], 2)

    def place(y_ref, k, tile, edges):
        for n in range(8):
            parity = core if n < 4 else 1 - core
            base = pl.multiple_of((2 * (n % 4) + parity) * PITCH + EDGE, 8)
            y_ref[k, pl.ds(base, STEP), :] = tile[n * STEP : (n + 1) * STEP]
        if edges:
            one, two = tile[ROWS : ROWS + EDGE], tile[ROWS + EDGE : ROWS + 2 * EDGE]
            y_ref[k, 0:EDGE, :] = jnp.where(core == 1, one, two)
            end = (SEG - 1) * PITCH + EDGE + STEP
            y_ref[k, end : end + EDGE, :] = jnp.where(core == 1, two, one)
            for s in range(SEG - 1):
                low, high = s * PITCH, (s + 1) * PITCH
                y_ref[k, high : high + EDGE, :] = y_ref[k, low + STEP : low + STEP + EDGE, :]
                y_ref[k, low + EDGE + STEP : low + 2 * EDGE + STEP, :] = y_ref[
                    k, high + EDGE : high + 2 * EDGE, :
                ]

    def take(y_ref, k, j):
        return y_ref[k, pl.ds(j + EDGE, SEG, stride=PITCH), :]

    return place, take


def gates_kernel(
    at_ref, own_ref, other_ref, h1_ref, h2_ref, gain_ref,
    rate_ref, ws_hbm, conv_hbm, bd_hbm, speed_hbm, extra_hbm,
    kd_out, xn_out, seg_out, send_out,
    ws_ref, conv_ref, bd_ref, speed_ref, extra_ref,
    xn_ref, y_ref, f_ref, g_ref, kd_ref, seg_ref, send_ref,
    ws_sem, table_sem, kd_sem, xn_sem, seg_sem, send_sem,
):
    place, take = placing(at_ref)
    ws_load = pltpu.make_async_copy(ws_hbm, ws_ref, ws_sem)
    ws_load.start()
    tables = ((conv_hbm, conv_ref), (bd_hbm, bd_ref), (speed_hbm, speed_ref), (extra_hbm, extra_ref))
    table_loads = [
        pltpu.make_async_copy(source, target, table_sem.at[n])
        for n, (source, target) in enumerate(tables)
    ]
    for load in table_loads:
        load.start()
    for n in range(4):
        normalize_shard(own_ref.at[n], gain_ref, xn_ref, n * STEP)
    for n, ref in enumerate((h1_ref, h2_ref)):
        normalize_shard(ref, gain_ref, xn_ref, ROWS + n * EDGE)
    for n in range(4):
        normalize_shard(other_ref.at[n], gain_ref, xn_ref, (n + 4) * STEP)
    xn_copy = pltpu.make_async_copy(xn_ref, xn_out, xn_sem)
    xn_copy.start()
    ws_load.wait()
    value = dot(xn_ref[...], ws_ref[...]).astype(BF16).astype(F32)
    for k in range(2):
        place(y_ref, k, value[:, k * 128 : (k + 1) * 128], True)
    for load in table_loads:
        load.wait()
    taps = conv_ref[...].astype(F32)

    def conv(i, _):
        rows = pl.ds(pl.multiple_of(i * 64, 64), 64)
        for lt in range(2):
            lanes = slice(lt * 128, lt * 128 + 128)
            near = [take(y_ref, lt, i * 8 + j - 2) for j in range(11)]
            out = []
            for j in range(8):
                value = taps[0:1, lanes] * near[j]
                for k in range(1, 4):
                    value = value + taps[k : k + 1, lanes] * near[j + k]
                out.append(value)
            f_ref[rows, lanes] = jnp.concatenate(out, axis=0).astype(BF16)
        return 0

    lax.fori_loop(0, STEP // 8, conv, 0)
    f = f_ref[...]
    for k in range(4):
        g_ref[:, k * 256 : (k + 1) * 256] = dot(f, bd_ref[:, k * 256 : (k + 1) * 256])

    def chunk(i, carry):
        rows = pl.ds(pl.multiple_of(i * 64, 64), 64)
        out = []
        for lt in range(2):
            hf, lf, hb, pb, lb = carry[lt]
            lanes = slice(lt * 128, lt * 128 + 128)
            wide = f_ref[rows, lanes].astype(F32)
            for d in range(2):
                col = d * 512 + lt * 128
                half = half_rate[d][:, lanes]
                recall = jnp.tanh(0.5 * g_ref[rows, col : col + 128])
                inlet = 0.5 * jnp.tanh(0.5 * g_ref[rows, col + 256 : col + 384]) + 0.5
                log_keep = half * recall + half + extra_ref[d, rows, :]
                keep = jnp.exp(log_keep)
                gap = (1.0 + keep * keep) * jnp.tanh(-log_keep)
                drive = gap * lax.rsqrt(jnp.maximum(gap, 1e-37)) * (inlet * wide)
                kd_ref[2 * d, rows, lanes] = keep
                kd_ref[2 * d + 1, rows, lanes] = drive
                for j in range(8):
                    kj = keep[8 * j : 8 * j + 8]
                    uj = drive[8 * j : 8 * j + 8]
                    lj = log_keep[8 * j : 8 * j + 8]
                    if d == 0:
                        hf = kj * hf + uj
                        lf = lf + lj
                    else:
                        hb = hb + pb * uj
                        pb = pb * kj
                        lb = lb + lj
            out.append((hf, lf, hb, pb, lb))
        return tuple(out)

    half_rate = [
        (-0.5 * FADING_FACTOR) * speed_ref[d : d + 1, 0:1] * rate_ref[d : d + 1, :] for d in range(2)
    ]
    zero = jnp.zeros((SEG, 128), F32)
    one = jnp.ones((SEG, 128), F32)
    totals = tuple((zero, zero, zero, one, zero) for _ in range(2))
    kd_copies = []
    for part in range(4):
        totals = lax.fori_loop(2 * part, 2 * part + 2, chunk, totals)
        rows = slice(part * 128, part * 128 + 128)
        copy = pltpu.make_async_copy(
            kd_ref.at[:, rows, :], kd_out.at[:, rows, :], kd_sem.at[part]
        )
        copy.start()
        kd_copies.append(copy)
    row = lax.broadcasted_iota(jnp.int32, (SEG, 128), 0)
    sends = [jnp.zeros((SEG, 128), F32), jnp.zeros((SEG, 128), F32)]
    for lt in range(2):
        hf, lf, hb, _, lb = totals[lt]
        lanes = slice(lt * 128, lt * 128 + 128)
        for d, (log_total, state) in enumerate(((lf, hf), (lb, hb))):
            factor = jnp.exp(log_total)
            for shift in (1, 2, 4):
                move = shift if d == 0 else SEG - shift
                inside = (row >= shift) if d == 0 else (row < SEG - shift)
                earlier_factor = jnp.where(inside, pltpu.roll(factor, move, 0), 1.0)
                earlier_state = jnp.where(inside, pltpu.roll(state, move, 0), 0.0)
                state = factor * earlier_state + state
                factor = factor * earlier_factor
            move = 1 if d == 0 else SEG - 1
            inside = (row >= 1) if d == 0 else (row < SEG - 1)
            seg_ref[2 * d, :, lanes] = jnp.where(inside, pltpu.roll(factor, move, 0), 1.0)
            seg_ref[2 * d + 1, :, lanes] = jnp.where(inside, pltpu.roll(state, move, 0), 0.0)
            end = SEG - 1 if d == 0 else 0
            whole_log = jnp.sum(log_total, axis=0, keepdims=True)
            whole_state = jnp.sum(jnp.where(row == end, state, 0.0), axis=0, keepdims=True)
            sends[d] = jnp.where(row == lt, whole_log, sends[d])
            sends[d] = jnp.where(row == 2 + lt, whole_state, sends[d])
    seg_copy = pltpu.make_async_copy(seg_ref, seg_out, seg_sem)
    seg_copy.start()
    shape = (1, 4, 128)
    forward, backward = (v[0:4].astype(BF16).reshape(shape) for v in sends)
    place_of = at_ref[0]
    for p in range(send_ref.shape[0]):
        send_ref[p : p + 1] = jnp.where(p > place_of, forward, backward)
    send_copy = pltpu.make_async_copy(send_ref, send_out, send_sem)
    send_copy.start()
    for copy in (xn_copy, seg_copy, *kd_copies, send_copy):
        copy.wait()


def pooling_kernel(
    at_ref, xn_hbm, wg_hbm, wp_hbm, cluster_ref, factor_ref,
    gate_ref, mix_ref,
    xn_ref, wg_ref, wp_ref, y_ref, pool_ref, p_ref, sem,
):
    loads = [
        pltpu.make_async_copy(source, target, sem.at[n])
        for n, (source, target) in enumerate(((xn_hbm, xn_ref), (wp_hbm, wp_ref), (wg_hbm, wg_ref)))
    ]
    for load in loads:
        load.start()
    place, take = placing(at_ref)
    position_of, column = at_ref[0], at_ref[1]
    total = at_ref[2]
    code = lax.rem(column, 4)
    loads[0].wait()
    loads[1].wait()
    xn = xn_ref[...]
    place(y_ref, 2, dot(xn, wp_ref[...]).astype(BF16).astype(F32), True)
    loads[2].wait()
    value = dot(xn, wg_ref[...]).astype(BF16).astype(F32)
    for k in range(2):
        place(y_ref, k, value[:, k * 128 : (k + 1) * 128], False)

    def gates(i, _):
        rows = pl.ds(pl.multiple_of(i * 64, 64), 64)
        for lt in range(2):
            tiles = [take(y_ref, lt, i * 8 + j) for j in range(8)]
            gate_ref[rows, lt * 128 : lt * 128 + 128] = jnp.concatenate(tiles, axis=0).astype(BF16)
        return 0

    lax.fori_loop(0, STEP // 8, gates, 0)

    def pools(i, _):
        rows = pl.ds(pl.multiple_of(i * 64, 64), 64)
        tiles = [take(y_ref, 2, i * 8 + j - EDGE) for j in range(8)]
        pool_ref[rows, :] = jnp.concatenate(tiles, axis=0)
        return 0

    lax.fori_loop(0, (STEP + 2 * EDGE) // 8, pools, 0)

    def windows(i, _):
        base = pl.multiple_of(i * 64, 64)
        level = pool_ref[pl.ds(base, 64 + 2 * EDGE * SEG), :]
        centre = level[EDGE * SEG : EDGE * SEG + 64]
        chosen = jnp.zeros((64, PC), F32)
        for k in range(4):
            shift = SEG << k
            size = level.shape[0] - shift
            level = level[:size] + level[shift:]
            begin = (EDGE - (1 << k)) * SEG
            chosen = jnp.where(code == k, level[begin : begin + 64], chosen)
        row = base + lax.broadcasted_iota(jnp.int32, (64, PC), 0)
        position = position_of * ROWS + (row & 7) * STEP + (row >> 3)
        reach = jnp.left_shift(1, code)
        count = jnp.minimum(position + reach, total) - jnp.maximum(position - reach, 0)
        p_ref[pl.ds(base, 64), :] = (chosen / count.astype(F32) - centre).astype(BF16)
        return 0

    lax.fori_loop(0, ROWS // 64, windows, 0)
    grouped = dot(p_ref[...], cluster_ref[...])
    mix_ref[...] = (grouped * factor_ref[...].astype(F32)).astype(BF16)


def states_kernel(
    at_ref, got_ref, seg_ref, kd_hbm, gate_ref, pool_mix_ref,
    send_ref, own_ref,
    kd_ref, hf_ref, hb_ref, mix_ref, kd_sem,
):
    loads = []
    for part in range(4):
        for n, at in enumerate((part, 3 - part)):
            there = (slice(2 * n, 2 * n + 2), slice(at * 128, at * 128 + 128), slice(None))
            loads.append(
                pltpu.make_async_copy(kd_hbm.at[there], kd_ref.at[there], kd_sem.at[2 * part + n])
            )
            loads[-1].start()
    place = at_ref[0]
    core = lax.rem(at_ref[1], 2)
    blocks = got_ref.shape[0]

    def arriving(i, carry):
        ahead, behind = carry
        for k in range(2):
            p = i * 2 + k
            v = got_ref[p].astype(F32)
            ahead = jnp.where(p < place, jnp.exp(v[0:2]) * ahead + v[2:4], ahead)
            p = blocks - 1 - p
            v = got_ref[p].astype(F32)
            behind = jnp.where(p > place, jnp.exp(v[0:2]) * behind + v[2:4], behind)
        return ahead, behind

    zero = jnp.zeros((2, 128), F32)
    carry = lax.fori_loop(0, blocks // 2, arriving, (zero, zero), unroll=min(8, blocks // 2))
    begin = []
    for lt in range(2):
        lanes = slice(lt * 128, lt * 128 + 128)
        for d in range(2):
            begin.append(
                seg_ref[2 * d, :, lanes] * carry[d][lt : lt + 1] + seg_ref[2 * d + 1, :, lanes]
            )

    def walk(i, carry):
        hf0, hb0, hf1, hb1 = carry
        for k in range(8):
            f = pl.ds(pl.multiple_of((i * 8 + k) * SEG, SEG), SEG)
            b = pl.ds(pl.multiple_of((STEP - 1 - i * 8 - k) * SEG, SEG), SEG)
            hf0 = kd_ref[0, f, 0:128] * hf0 + kd_ref[1, f, 0:128]
            hf1 = kd_ref[0, f, 128:256] * hf1 + kd_ref[1, f, 128:256]
            hb0 = kd_ref[2, b, 0:128] * hb0 + kd_ref[3, b, 0:128]
            hb1 = kd_ref[2, b, 128:256] * hb1 + kd_ref[3, b, 128:256]
            hf_ref[f, 0:128] = hf0
            hf_ref[f, 128:256] = hf1
            hb_ref[b, 0:128] = hb0
            hb_ref[b, 128:256] = hb1
        return hf0, hb0, hf1, hb1

    states = tuple(begin)
    for part in range(4):
        loads[2 * part].wait()
        loads[2 * part + 1].wait()
        states = lax.fori_loop(2 * part, 2 * part + 2, walk, states)

    def mixing(i, _):
        rows = pl.ds(pl.multiple_of(i * 64, 64), 64)
        for lt in range(2):
            lanes = slice(lt * 128, lt * 128 + 128)
            v = gate_ref[rows, lanes].astype(F32)
            inner = 0.7978845608028654 * (v + 0.044715 * (v * v * v))
            act = v * (0.5 * (1.0 + jnp.tanh(inner)))
            mix_ref[lt, rows, :] = act * (hf_ref[rows, lanes] + hb_ref[rows, lanes])
        mix_ref[2, rows, :] = pool_mix_ref[rows, :].astype(F32)
        return 0

    lax.fori_loop(0, ROWS // 64, mixing, 0)
    for x in range(4):
        rows = slice(x * STEP, (x + 1) * STEP)
        for k in range(3):
            lanes = slice(k * 128, k * 128 + 128)
            there = mix_ref[k, pl.ds(2 * x + 1 - core, STEP, stride=SEG), :]
            send_ref[rows, lanes] = there.astype(BF16)
            here = mix_ref[k, pl.ds(2 * x + core, STEP, stride=SEG), :]
            own_ref[rows, lanes] = here.astype(BF16)


def output_kernel(
    own_ref, got_ref, wr_hbm, wp_hbm, vr_hbm, vp_hbm, out_ref, wr_ref, wp_ref, vr_ref, vp_ref, sem
):
    pairs = ((wr_hbm, wr_ref), (wp_hbm, wp_ref), (vr_hbm, vr_ref), (vp_hbm, vp_ref))
    copies = []
    for k in range(4):
        lanes = slice(k * 512, k * 512 + 512)
        copies.append(
            [
                pltpu.make_async_copy(source.at[:, lanes], target.at[:, lanes], sem.at[k, n])
                for n, (source, target) in enumerate(pairs)
            ]
        )
        for copy in copies[k]:
            copy.start()
    own_state = own_ref[:, 0:CH]
    own_pool = own_ref[:, CH : CH + PC]
    got_state = got_ref[:, 0:CH]
    got_pool = got_ref[:, CH : CH + PC]
    for k in range(4):
        lanes = slice(k * 512, k * 512 + 512)
        for copy in copies[k]:
            copy.wait()
        value = dot(own_state, wr_ref[:, lanes]) + dot(got_state, vr_ref[:, lanes])
        value = value + dot(own_pool, wp_ref[:, lanes]) + dot(got_pool, vp_ref[:, lanes])
        value = value.astype(BF16)
        for x in range(4):
            out_ref[x, :, lanes] = value[x * STEP : (x + 1) * STEP]


def local(
    incoming_activity,
    entry_standardize_factor,
    recursive_entry_matrix,
    final_switch_matrix,
    averaging_entry_matrix,
    percolumn_filter_coefficients,
    switch_tiled_matrices,
    prior_fading_odds,
    speed_factors,
    extra_fading_amounts,
    averaging_cluster_matrices,
    averaging_feature_factor,
    recursive_final_matrix,
    averaging_final_matrix,
):
    blocks = lax.axis_size("sp")
    place = lax.axis_index("sp")
    column = lax.axis_index("tp")
    core = column % 2
    same_core = [[0, 2, 4, 6], [1, 3, 5, 7]]
    sibling = [(k, k ^ 1) for k in range(8)]

    def exchange(v):
        return lax.all_to_all(
            v, "tp", split_axis=0, concat_axis=0, tiled=True, axis_index_groups=same_core
        )

    def edge_pairs(cross):
        pairs = []
        for sp in range(blocks):
            for tp in range(8):
                to = sp + 1 if tp % 2 else sp - 1
                if 0 <= to < blocks:
                    pairs.append((sp * 8 + tp, to * 8 + (tp ^ cross)))
        return pairs

    def to_sibling(v):
        return lax.ppermute(v, "tp", sibling)

    smem = pl.BlockSpec(memory_space=pltpu.SMEM)
    at = jnp.stack([place, column, jnp.asarray(blocks * ROWS)]).astype(jnp.int32)
    spread = pl.pallas_call(
        spread_kernel,
        out_shape=HBM((4, STEP, WIDE), BF16),
        in_specs=hspecs(1),
        out_specs=pl.BlockSpec(memory_space=HBM),
        scratch_shapes=[VMEM((STEP, WIDE), BF16), DMA, DMA((4,))],
        compiler_params=params(2),
        cost_estimate=cost(0, 1_300_000),
        name="spread",
    )(*kept(incoming_activity))
    x_own = exchange(spread)
    sibling_recursive = lax.ppermute(recursive_final_matrix, "tp", sibling)
    sibling_averaging = lax.ppermute(averaging_final_matrix, "tp", sibling)
    x_other = to_sibling(x_own)
    edge = lax.dynamic_slice(
        x_own, (3 * core, (STEP - EDGE) * core, 0), (1, EDGE, WIDE)
    ).reshape(EDGE, WIDE)
    edge_same = lax.ppermute(edge, ("sp", "tp"), edge_pairs(0))
    edge_cross = lax.ppermute(edge, ("sp", "tp"), edge_pairs(1))

    at = jnp.stack([place, column, jnp.asarray(blocks * ROWS)]).astype(jnp.int32)
    gain = entry_standardize_factor.reshape(1, WIDE)
    rate = jax.nn.softplus(-prior_fading_odds)
    maps, extra = pl.pallas_call(
        tables_kernel,
        out_shape=(
            HBM((CH, 4 * CH), BF16),
            HBM((2, ROWS, 128), F32),
        ),
        in_specs=vspecs(2),
        out_specs=tuple(vspecs(2)),
        compiler_params=params(4),
        cost_estimate=cost(1_000_000, 2_000_000),
        name="tables",
    )(switch_tiled_matrices, extra_fading_amounts.reshape(2, SEG, STEP))

    kd, xn, seg, send = pl.pallas_call(
        gates_kernel,
        out_shape=(
            HBM((4, ROWS, CH), F32),
            HBM((ROWS + 2 * EDGE, WIDE), BF16),
            HBM((4, SEG, CH), F32),
            HBM((blocks, 4, 128), BF16),
        ),
        in_specs=[smem, *vspecs(6), *hspecs(5)],
        out_specs=tuple(hspecs(4)),
        scratch_shapes=[
            VMEM((WIDE, CH), BF16),
            VMEM((4, CH), BF16),
            VMEM((CH, 4 * CH), BF16),
            VMEM((2, ROWS), F32),
            VMEM((2, ROWS, 128), F32),
            VMEM((ROWS + 2 * EDGE, WIDE), BF16),
            VMEM((2, SEG * PITCH, 128), F32),
            VMEM((ROWS, CH), BF16),
            VMEM((ROWS, 4 * CH), F32),
            VMEM((4, ROWS, CH), F32),
            VMEM((4, SEG, CH), F32),
            VMEM((blocks, 4, 128), BF16),
            DMA,
            DMA((4,)),
            DMA((4,)),
            DMA,
            DMA,
            DMA,
        ],
        compiler_params=params(20),
        cost_estimate=cost(2 * 528 * WIDE * 256, 8_000_000, 1_000_000),
        name="gates",
    )(
        at, x_own, x_other, edge_same, edge_cross, gain, rate,
        *kept(recursive_entry_matrix, percolumn_filter_coefficients, maps, speed_factors, extra),
    )

    got = lax.all_to_all(send, "sp", split_axis=0, concat_axis=0, tiled=True)

    gate, pool_mix = pl.pallas_call(
        pooling_kernel,
        out_shape=(
            jax.ShapeDtypeStruct((ROWS, CH), BF16),
            jax.ShapeDtypeStruct((ROWS, PC), BF16),
        ),
        in_specs=[smem, *hspecs(3), *vspecs(2)],
        out_specs=tuple(vspecs(2)),
        scratch_shapes=[
            VMEM((ROWS + 2 * EDGE, WIDE), BF16),
            VMEM((WIDE, CH), BF16),
            VMEM((WIDE, PC), BF16),
            VMEM((3, SEG * PITCH, 128), F32),
            VMEM((ROWS + 2 * EDGE * SEG, PC), F32),
            VMEM((ROWS, PC), BF16),
            DMA((3,)),
        ],
        compiler_params=params(16),
        cost_estimate=cost(8 * 528 * WIDE * 384, 8_000_000, 200_000),
        name="pooling",
    )(
        at, *kept(xn, final_switch_matrix, averaging_entry_matrix),
        averaging_cluster_matrices.reshape(PC, PC), averaging_feature_factor.reshape(1, PC),
    )

    mix_send, mix_own = pl.pallas_call(
        states_kernel,
        out_shape=(
            jax.ShapeDtypeStruct((256, CH + PC), BF16),
            jax.ShapeDtypeStruct((256, CH + PC), BF16),
        ),
        in_specs=[smem, *vspecs(2), *hspecs(1), *vspecs(2)],
        out_specs=tuple(vspecs(2)),
        scratch_shapes=[
            VMEM((4, ROWS, CH), F32),
            VMEM((ROWS, CH), F32),
            VMEM((ROWS, CH), F32),
            VMEM((3, ROWS, 128), F32),
            DMA((8,)),
        ],
        compiler_params=params(8),
        cost_estimate=cost(1_000_000_000, 4_000_000, 100_000),
        name="states",
    )(at, got, seg, *kept(kd), gate, pool_mix)

    mix_got = lax.ppermute(mix_send, "tp", sibling)

    partial = pl.pallas_call(
        output_kernel,
        out_shape=jax.ShapeDtypeStruct((4, STEP, WIDE), BF16),
        in_specs=[*vspecs(2), *hspecs(4)],
        out_specs=pl.BlockSpec(memory_space=VMEM),
        scratch_shapes=[
            VMEM((CH, WIDE), BF16),
            VMEM((PC, WIDE), BF16),
            VMEM((CH, WIDE), BF16),
            VMEM((PC, WIDE), BF16),
            DMA((4, 4)),
        ],
        compiler_params=params(10),
        cost_estimate=cost(4 * 256 * 384 * WIDE, 5_000_000),
        name="output",
    )(
        mix_own,
        mix_got,
        *kept(recursive_final_matrix, averaging_final_matrix, sibling_recursive, sibling_averaging),
    )
    moved = exchange(partial)
    return jnp.sum(moved.astype(F32), axis=0).astype(BF16)


def solution(mesh):
    in_specs = (
        P(("sp", "tp"), None),
        P(),
        P(None, "tp"),
        P(None, "tp"),
        P(None, "tp"),
        P(None, "tp"),
        P(None, None, "tp", None, None),
        P(None, "tp"),
        P(None, "sp"),
        P(None, "sp"),
        P("tp", None, None),
        P("tp"),
        P("tp", None),
        P("tp", None),
    )
    out_specs = P(("sp", "tp"), None)


    return jax.shard_map(local, mesh=mesh, in_specs=in_specs, out_specs=out_specs, check_vma=False)
```

```python
import jax
import jax.numpy as jnp
from jax import lax
from jax.experimental import pallas as pl
from jax.experimental.pallas import tpu as pltpu
from jax.sharding import PartitionSpec as P

FADING_FACTOR = 8.0
epsilon = 1e-06

SEG = 8
STEP = 64
ROWS = SEG * STEP
EDGE = 8
WIDE = 2048
CH = 256
PC = 128
F32 = jnp.float32
BF16 = jnp.bfloat16
VMEM = pltpu.VMEM
HBM = pltpu.HBM
DMA = pltpu.SemaphoreType.DMA
PITCH = STEP + 3 * EDGE


def vspecs(n):
    return [pl.BlockSpec(memory_space=VMEM)] * n


def hspecs(n):
    return [pl.BlockSpec(memory_space=HBM)] * n


def kept(*arrays):
    return [pltpu.with_memory_space_constraint(array, HBM) for array in arrays]


def params(mebibytes):
    return pltpu.CompilerParams(vmem_limit_bytes=mebibytes * 1024 * 1024)


def cost(flops, nbytes, trans=0):
    return pl.CostEstimate(flops=flops, bytes_accessed=nbytes, transcendentals=trans)


def dot(a, b):
    return jnp.dot(a, b, preferred_element_type=F32)


def normalize(read, write, gain_ref, rows):
    total = jnp.zeros((rows, 128), F32)
    for k in range(WIDE // 128):
        v = read(k * 128).astype(F32)
        total = total + v * v
    inv = lax.rsqrt(jnp.sum(total, axis=1, keepdims=True) * (1.0 / WIDE) + epsilon)
    for k in range(WIDE // 128):
        v = read(k * 128).astype(F32)
        gain = gain_ref[0:1, k * 128 : (k + 1) * 128].astype(F32)
        write(k * 128, ((v * inv) * gain).astype(BF16))


def normalize_shard(x_ref, gain_ref, out_ref, base):
    def read(lane):
        return x_ref[:, lane : lane + 128]

    def write(lane, v):
        out_ref[base : base + x_ref.shape[0], lane : lane + 128] = v

    normalize(read, write, gain_ref, x_ref.shape[0])


def spread_kernel(x_ref, out_ref, held_ref, in_sem, out_sem):
    load = pltpu.make_async_copy(x_ref, held_ref, in_sem)
    load.start()
    load.wait()
    copies = [pltpu.make_async_copy(held_ref, out_ref.at[k], out_sem.at[k]) for k in range(4)]
    for copy in copies:
        copy.start()
    for copy in copies:
        copy.wait()


def tables_kernel(maps_ref, extra_ref, bd_ref, spread_ref):
    bd_ref[...] = jnp.zeros_like(bd_ref)
    blank = jnp.zeros((64, 64), BF16)
    for d in range(2):
        for q in range(2):
            for b in range(4):
                block = maps_ref[d, q, b]
                tile = jnp.concatenate([block, blank] if b % 2 == 0 else [blank, block], axis=1)
                col = (d * 2 + q) * CH + (b // 2) * 128
                bd_ref[b * 64 : b * 64 + 64, col : col + 128] = tile
    for d in range(2):
        for j in range(STEP):
            spread_ref[d, j * SEG : (j + 1) * SEG, :] = jnp.broadcast_to(
                extra_ref[d, :, j : j + 1], (SEG, 128)
            )


def placing(at_ref):
    core = lax.rem(at_ref[1], 2)

    def place(y_ref, k, tile, edges):
        for n in range(8):
            parity = core if n < 4 else 1 - core
            base = pl.multiple_of((2 * (n % 4) + parity) * PITCH + EDGE, 8)
            y_ref[k, pl.ds(base, STEP), :] = tile[n * STEP : (n + 1) * STEP]
        if edges:
            one, two = tile[ROWS : ROWS + EDGE], tile[ROWS + EDGE : ROWS + 2 * EDGE]
            y_ref[k, 0:EDGE, :] = jnp.where(core == 1, one, two)
            end = (SEG - 1) * PITCH + EDGE + STEP
            y_ref[k, end : end + EDGE, :] = jnp.where(core == 1, two, one)
            for s in range(SEG - 1):
                low, high = s * PITCH, (s + 1) * PITCH
                y_ref[k, high : high + EDGE, :] = y_ref[k, low + STEP : low + STEP + EDGE, :]
                y_ref[k, low + EDGE + STEP : low + 2 * EDGE + STEP, :] = y_ref[
                    k, high + EDGE : high + 2 * EDGE, :
                ]

    def take(y_ref, k, j):
        return y_ref[k, pl.ds(j + EDGE, SEG, stride=PITCH), :]

    return place, take


def gates_kernel(
    at_ref, own_ref, other_ref, h1_ref, h2_ref, gain_ref,
    rate_ref, ws_hbm, conv_hbm, bd_hbm, speed_hbm, extra_hbm,
    kd_out, xn_out, seg_out, send_out,
    ws_ref, conv_ref, bd_ref, speed_ref, extra_ref,
    xn_ref, y_ref, f_ref, g_ref, kd_ref, seg_ref, send_ref,
    ws_sem, table_sem, kd_sem, xn_sem, seg_sem, send_sem,
):
    place, take = placing(at_ref)
    ws_load = pltpu.make_async_copy(ws_hbm, ws_ref, ws_sem)
    ws_load.start()
    tables = ((conv_hbm, conv_ref), (bd_hbm, bd_ref), (speed_hbm, speed_ref), (extra_hbm, extra_ref))
    table_loads = [
        pltpu.make_async_copy(source, target, table_sem.at[n])
        for n, (source, target) in enumerate(tables)
    ]
    for load in table_loads:
        load.start()
    for n in range(4):
        normalize_shard(own_ref.at[n], gain_ref, xn_ref, n * STEP)
    for n, ref in enumerate((h1_ref, h2_ref)):
        normalize_shard(ref, gain_ref, xn_ref, ROWS + n * EDGE)
    for n in range(4):
        normalize_shard(other_ref.at[n], gain_ref, xn_ref, (n + 4) * STEP)
    xn_copy = pltpu.make_async_copy(xn_ref, xn_out, xn_sem)
    xn_copy.start()
    ws_load.wait()
    value = dot(xn_ref[...], ws_ref[...]).astype(BF16).astype(F32)
    for k in range(2):
        place(y_ref, k, value[:, k * 128 : (k + 1) * 128], True)
    for load in table_loads:
        load.wait()
    taps = conv_ref[...].astype(F32)

    def conv(i, _):
        rows = pl.ds(pl.multiple_of(i * 64, 64), 64)
        for lt in range(2):
            lanes = slice(lt * 128, lt * 128 + 128)
            near = [take(y_ref, lt, i * 8 + j - 2) for j in range(11)]
            out = []
            for j in range(8):
                value = taps[0:1, lanes] * near[j]
                for k in range(1, 4):
                    value = value + taps[k : k + 1, lanes] * near[j + k]
                out.append(value)
            f_ref[rows, lanes] = jnp.concatenate(out, axis=0).astype(BF16)
        return 0

    lax.fori_loop(0, STEP // 8, conv, 0)
    f = f_ref[...]
    for k in range(4):
        g_ref[:, k * 256 : (k + 1) * 256] = dot(f, bd_ref[:, k * 256 : (k + 1) * 256])

    def chunk(i, carry):
        rows = pl.ds(pl.multiple_of(i * 64, 64), 64)
        out = []
        for lt in range(2):
            hf, lf, hb, pb, lb = carry[lt]
            lanes = slice(lt * 128, lt * 128 + 128)
            wide = f_ref[rows, lanes].astype(F32)
            for d in range(2):
                col = d * 512 + lt * 128
                half = half_rate[d][:, lanes]
                recall = jnp.tanh(0.5 * g_ref[rows, col : col + 128])
                inlet = 0.5 * jnp.tanh(0.5 * g_ref[rows, col + 256 : col + 384]) + 0.5
                log_keep = half * recall + half + extra_ref[d, rows, :]
                keep = jnp.exp(log_keep)
                gap = (1.0 + keep * keep) * jnp.tanh(-log_keep)
                drive = gap * lax.rsqrt(jnp.maximum(gap, 1e-37)) * (inlet * wide)
                kd_ref[2 * d, rows, lanes] = keep
                kd_ref[2 * d + 1, rows, lanes] = drive
                for j in range(8):
                    kj = keep[8 * j : 8 * j + 8]
                    uj = drive[8 * j : 8 * j + 8]
                    lj = log_keep[8 * j : 8 * j + 8]
                    if d == 0:
                        hf = kj * hf + uj
                        lf = lf + lj
                    else:
                        hb = hb + pb * uj
                        pb = pb * kj
                        lb = lb + lj
            out.append((hf, lf, hb, pb, lb))
        return tuple(out)

    half_rate = [
        (-0.5 * FADING_FACTOR) * speed_ref[d : d + 1, 0:1] * rate_ref[d : d + 1, :] for d in range(2)
    ]
    zero = jnp.zeros((SEG, 128), F32)
    one = jnp.ones((SEG, 128), F32)
    totals = tuple((zero, zero, zero, one, zero) for _ in range(2))
    kd_copies = []
    for part in range(4):
        totals = lax.fori_loop(2 * part, 2 * part + 2, chunk, totals)
        rows = slice(part * 128, part * 128 + 128)
        copy = pltpu.make_async_copy(
            kd_ref.at[:, rows, :], kd_out.at[:, rows, :], kd_sem.at[part]
        )
        copy.start()
        kd_copies.append(copy)
    row = lax.broadcasted_iota(jnp.int32, (SEG, 128), 0)
    sends = [jnp.zeros((SEG, 128), F32), jnp.zeros((SEG, 128), F32)]
    for lt in range(2):
        hf, lf, hb, _, lb = totals[lt]
        lanes = slice(lt * 128, lt * 128 + 128)
        for d, (log_total, state) in enumerate(((lf, hf), (lb, hb))):
            factor = jnp.exp(log_total)
            for shift in (1, 2, 4):
                move = shift if d == 0 else SEG - shift
                inside = (row >= shift) if d == 0 else (row < SEG - shift)
                earlier_factor = jnp.where(inside, pltpu.roll(factor, move, 0), 1.0)
                earlier_state = jnp.where(inside, pltpu.roll(state, move, 0), 0.0)
                state = factor * earlier_state + state
                factor = factor * earlier_factor
            move = 1 if d == 0 else SEG - 1
            inside = (row >= 1) if d == 0 else (row < SEG - 1)
            seg_ref[2 * d, :, lanes] = jnp.where(inside, pltpu.roll(factor, move, 0), 1.0)
            seg_ref[2 * d + 1, :, lanes] = jnp.where(inside, pltpu.roll(state, move, 0), 0.0)
            end = SEG - 1 if d == 0 else 0
            whole_log = jnp.sum(log_total, axis=0, keepdims=True)
            whole_state = jnp.sum(jnp.where(row == end, state, 0.0), axis=0, keepdims=True)
            sends[d] = jnp.where(row == lt, whole_log, sends[d])
            sends[d] = jnp.where(row == 2 + lt, whole_state, sends[d])
    seg_copy = pltpu.make_async_copy(seg_ref, seg_out, seg_sem)
    seg_copy.start()
    shape = (1, 4, 128)
    forward, backward = (v[0:4].astype(BF16).reshape(shape) for v in sends)
    place_of = at_ref[0]
    for p in range(send_ref.shape[0]):
        send_ref[p : p + 1] = jnp.where(p > place_of, forward, backward)
    send_copy = pltpu.make_async_copy(send_ref, send_out, send_sem)
    send_copy.start()
    for copy in (xn_copy, seg_copy, *kd_copies, send_copy):
        copy.wait()


def pooling_kernel(
    at_ref, xn_hbm, wg_hbm, wp_hbm, cluster_ref, factor_ref,
    gate_ref, mix_ref,
    xn_ref, wg_ref, wp_ref, y_ref, pool_ref, p_ref, sem,
):
    loads = [
        pltpu.make_async_copy(source, target, sem.at[n])
        for n, (source, target) in enumerate(((xn_hbm, xn_ref), (wp_hbm, wp_ref), (wg_hbm, wg_ref)))
    ]
    for load in loads:
        load.start()
    place, take = placing(at_ref)
    position_of, column = at_ref[0], at_ref[1]
    total = at_ref[2]
    code = lax.rem(column, 4)
    loads[0].wait()
    loads[1].wait()
    xn = xn_ref[...]
    place(y_ref, 2, dot(xn, wp_ref[...]).astype(BF16).astype(F32), True)
    loads[2].wait()
    value = dot(xn, wg_ref[...]).astype(BF16).astype(F32)
    for k in range(2):
        place(y_ref, k, value[:, k * 128 : (k + 1) * 128], False)

    def gates(i, _):
        rows = pl.ds(pl.multiple_of(i * 64, 64), 64)
        for lt in range(2):
            tiles = [take(y_ref, lt, i * 8 + j) for j in range(8)]
            gate_ref[rows, lt * 128 : lt * 128 + 128] = jnp.concatenate(tiles, axis=0).astype(BF16)
        return 0

    lax.fori_loop(0, STEP // 8, gates, 0)

    def pools(i, _):
        rows = pl.ds(pl.multiple_of(i * 64, 64), 64)
        tiles = [take(y_ref, 2, i * 8 + j - EDGE) for j in range(8)]
        pool_ref[rows, :] = jnp.concatenate(tiles, axis=0)
        return 0

    lax.fori_loop(0, (STEP + 2 * EDGE) // 8, pools, 0)

    def windows(i, _):
        base = pl.multiple_of(i * 64, 64)
        level = pool_ref[pl.ds(base, 64 + 2 * EDGE * SEG), :]
        centre = level[EDGE * SEG : EDGE * SEG + 64]
        chosen = jnp.zeros((64, PC), F32)
        for k in range(4):
            shift = SEG << k
            size = level.shape[0] - shift
            level = level[:size] + level[shift:]
            begin = (EDGE - (1 << k)) * SEG
            chosen = jnp.where(code == k, level[begin : begin + 64], chosen)
        row = base + lax.broadcasted_iota(jnp.int32, (64, PC), 0)
        position = position_of * ROWS + (row & 7) * STEP + (row >> 3)
        reach = jnp.left_shift(1, code)
        count = jnp.minimum(position + reach, total) - jnp.maximum(position - reach, 0)
        p_ref[pl.ds(base, 64), :] = (chosen / count.astype(F32) - centre).astype(BF16)
        return 0

    lax.fori_loop(0, ROWS // 64, windows, 0)
    grouped = dot(p_ref[...], cluster_ref[...])
    mix_ref[...] = (grouped * factor_ref[...].astype(F32)).astype(BF16)


def states_kernel(
    at_ref, got_ref, seg_ref, kd_hbm, gate_ref, pool_mix_ref,
    send_ref, own_ref,
    kd_ref, hf_ref, hb_ref, mix_ref, kd_sem,
):
    loads = []
    for part in range(4):
        for n, at in enumerate((part, 3 - part)):
            there = (slice(2 * n, 2 * n + 2), slice(at * 128, at * 128 + 128), slice(None))
            loads.append(
                pltpu.make_async_copy(kd_hbm.at[there], kd_ref.at[there], kd_sem.at[2 * part + n])
            )
            loads[-1].start()
    place = at_ref[0]
    core = lax.rem(at_ref[1], 2)
    blocks = got_ref.shape[0]

    def arriving(i, carry):
        ahead, behind = carry
        for k in range(2):
            p = i * 2 + k
            v = got_ref[p].astype(F32)
            ahead = jnp.where(p < place, jnp.exp(v[0:2]) * ahead + v[2:4], ahead)
            p = blocks - 1 - p
            v = got_ref[p].astype(F32)
            behind = jnp.where(p > place, jnp.exp(v[0:2]) * behind + v[2:4], behind)
        return ahead, behind

    zero = jnp.zeros((2, 128), F32)
    carry = lax.fori_loop(0, blocks // 2, arriving, (zero, zero), unroll=min(8, blocks // 2))
    begin = []
    for lt in range(2):
        lanes = slice(lt * 128, lt * 128 + 128)
        for d in range(2):
            begin.append(
                seg_ref[2 * d, :, lanes] * carry[d][lt : lt + 1] + seg_ref[2 * d + 1, :, lanes]
            )

    def walk(i, carry):
        hf0, hb0, hf1, hb1 = carry
        for k in range(8):
            f = pl.ds(pl.multiple_of((i * 8 + k) * SEG, SEG), SEG)
            b = pl.ds(pl.multiple_of((STEP - 1 - i * 8 - k) * SEG, SEG), SEG)
            hf0 = kd_ref[0, f, 0:128] * hf0 + kd_ref[1, f, 0:128]
            hf1 = kd_ref[0, f, 128:256] * hf1 + kd_ref[1, f, 128:256]
            hb0 = kd_ref[2, b, 0:128] * hb0 + kd_ref[3, b, 0:128]
            hb1 = kd_ref[2, b, 128:256] * hb1 + kd_ref[3, b, 128:256]
            hf_ref[f, 0:128] = hf0
            hf_ref[f, 128:256] = hf1
            hb_ref[b, 0:128] = hb0
            hb_ref[b, 128:256] = hb1
        return hf0, hb0, hf1, hb1

    states = tuple(begin)
    for part in range(4):
        loads[2 * part].wait()
        loads[2 * part + 1].wait()
        states = lax.fori_loop(2 * part, 2 * part + 2, walk, states)

    def mixing(i, _):
        rows = pl.ds(pl.multiple_of(i * 64, 64), 64)
        for lt in range(2):
            lanes = slice(lt * 128, lt * 128 + 128)
            v = gate_ref[rows, lanes].astype(F32)
            inner = 0.7978845608028654 * (v + 0.044715 * (v * v * v))
            act = v * (0.5 * (1.0 + jnp.tanh(inner)))
            mix_ref[lt, rows, :] = act * (hf_ref[rows, lanes] + hb_ref[rows, lanes])
        mix_ref[2, rows, :] = pool_mix_ref[rows, :].astype(F32)
        return 0

    lax.fori_loop(0, ROWS // 64, mixing, 0)
    for x in range(4):
        rows = slice(x * STEP, (x + 1) * STEP)
        for k in range(3):
            lanes = slice(k * 128, k * 128 + 128)
            there = mix_ref[k, pl.ds(2 * x + 1 - core, STEP, stride=SEG), :]
            send_ref[rows, lanes] = there.astype(BF16)
            here = mix_ref[k, pl.ds(2 * x + core, STEP, stride=SEG), :]
            own_ref[rows, lanes] = here.astype(BF16)


def weights_in_parts(pairs, sem):
    waits = []
    for k in range(4):
        lanes = slice(k * 512, k * 512 + 512)
        copies = [
            pltpu.make_async_copy(source.at[:, lanes], target.at[:, lanes], sem.at[k, n])
            for n, (source, target) in enumerate(pairs)
        ]
        for copy in copies:
            copy.start()
        waits.append(copies)
    return waits


def own_output_kernel(own_ref, wr_hbm, wp_hbm, out_ref, wr_ref, wp_ref, sem):
    waits = weights_in_parts(((wr_hbm, wr_ref), (wp_hbm, wp_ref)), sem)
    for k in range(4):
        lanes = slice(k * 512, k * 512 + 512)
        for copy in waits[k]:
            copy.wait()
        out_ref[:, lanes] = dot(own_ref[:, 0:CH], wr_ref[:, lanes]) + dot(
            own_ref[:, CH : CH + PC], wp_ref[:, lanes]
        )


def output_kernel(own_ref, got_ref, vr_ref, vp_ref, out_ref):
    for k in range(4):
        lanes = slice(k * 512, k * 512 + 512)
        value = dot(got_ref[:, 0:CH], vr_ref[:, lanes])
        value = value + dot(got_ref[:, CH : CH + PC], vp_ref[:, lanes])
        value = (value + own_ref[:, lanes]).astype(BF16)
        for x in range(4):
            out_ref[x, :, lanes] = value[x * STEP : (x + 1) * STEP]


def local(
    incoming_activity,
    entry_standardize_factor,
    recursive_entry_matrix,
    final_switch_matrix,
    averaging_entry_matrix,
    percolumn_filter_coefficients,
    switch_tiled_matrices,
    prior_fading_odds,
    speed_factors,
    extra_fading_amounts,
    averaging_cluster_matrices,
    averaging_feature_factor,
    recursive_final_matrix,
    averaging_final_matrix,
):
    blocks = lax.axis_size("sp")
    place = lax.axis_index("sp")
    column = lax.axis_index("tp")
    core = column % 2
    same_core = [[0, 2, 4, 6], [1, 3, 5, 7]]
    sibling = [(k, k ^ 1) for k in range(8)]

    def exchange(v):
        return lax.all_to_all(
            v, "tp", split_axis=0, concat_axis=0, tiled=True, axis_index_groups=same_core
        )

    def edge_pairs(cross):
        pairs = []
        for sp in range(blocks):
            for tp in range(8):
                to = sp + 1 if tp % 2 else sp - 1
                if 0 <= to < blocks:
                    pairs.append((sp * 8 + tp, to * 8 + (tp ^ cross)))
        return pairs

    def to_sibling(v):
        return lax.ppermute(v, "tp", sibling)

    smem = pl.BlockSpec(memory_space=pltpu.SMEM)
    at = jnp.stack([place, column, jnp.asarray(blocks * ROWS)]).astype(jnp.int32)
    spread = pl.pallas_call(
        spread_kernel,
        out_shape=HBM((4, STEP, WIDE), BF16),
        in_specs=hspecs(1),
        out_specs=pl.BlockSpec(memory_space=HBM),
        scratch_shapes=[VMEM((STEP, WIDE), BF16), DMA, DMA((4,))],
        compiler_params=params(2),
        cost_estimate=cost(0, 1_300_000),
        name="spread",
    )(*kept(incoming_activity))
    x_own = exchange(spread)
    sibling_recursive = lax.ppermute(recursive_final_matrix, "tp", sibling)
    sibling_averaging = lax.ppermute(averaging_final_matrix, "tp", sibling)
    x_other = to_sibling(x_own)
    edge = lax.dynamic_slice(
        x_own, (3 * core, (STEP - EDGE) * core, 0), (1, EDGE, WIDE)
    ).reshape(EDGE, WIDE)
    edge_same = lax.ppermute(edge, ("sp", "tp"), edge_pairs(0))
    edge_cross = lax.ppermute(edge, ("sp", "tp"), edge_pairs(1))

    at = jnp.stack([place, column, jnp.asarray(blocks * ROWS)]).astype(jnp.int32)
    gain = entry_standardize_factor.reshape(1, WIDE)
    rate = jax.nn.softplus(-prior_fading_odds)
    maps, extra = pl.pallas_call(
        tables_kernel,
        out_shape=(
            HBM((CH, 4 * CH), BF16),
            HBM((2, ROWS, 128), F32),
        ),
        in_specs=vspecs(2),
        out_specs=tuple(vspecs(2)),
        compiler_params=params(4),
        cost_estimate=cost(1_000_000, 2_000_000),
        name="tables",
    )(switch_tiled_matrices, extra_fading_amounts.reshape(2, SEG, STEP))

    kd, xn, seg, send = pl.pallas_call(
        gates_kernel,
        out_shape=(
            HBM((4, ROWS, CH), F32),
            HBM((ROWS + 2 * EDGE, WIDE), BF16),
            HBM((4, SEG, CH), F32),
            HBM((blocks, 4, 128), BF16),
        ),
        in_specs=[smem, *vspecs(6), *hspecs(5)],
        out_specs=tuple(hspecs(4)),
        scratch_shapes=[
            VMEM((WIDE, CH), BF16),
            VMEM((4, CH), BF16),
            VMEM((CH, 4 * CH), BF16),
            VMEM((2, ROWS), F32),
            VMEM((2, ROWS, 128), F32),
            VMEM((ROWS + 2 * EDGE, WIDE), BF16),
            VMEM((2, SEG * PITCH, 128), F32),
            VMEM((ROWS, CH), BF16),
            VMEM((ROWS, 4 * CH), F32),
            VMEM((4, ROWS, CH), F32),
            VMEM((4, SEG, CH), F32),
            VMEM((blocks, 4, 128), BF16),
            DMA,
            DMA((4,)),
            DMA((4,)),
            DMA,
            DMA,
            DMA,
        ],
        compiler_params=params(20),
        cost_estimate=cost(2 * 528 * WIDE * 256, 8_000_000, 1_000_000),
        name="gates",
    )(
        at, x_own, x_other, edge_same, edge_cross, gain, rate,
        *kept(recursive_entry_matrix, percolumn_filter_coefficients, maps, speed_factors, extra),
    )

    got = lax.all_to_all(send, "sp", split_axis=0, concat_axis=0, tiled=True)

    gate, pool_mix = pl.pallas_call(
        pooling_kernel,
        out_shape=(
            jax.ShapeDtypeStruct((ROWS, CH), BF16),
            jax.ShapeDtypeStruct((ROWS, PC), BF16),
        ),
        in_specs=[smem, *hspecs(3), *vspecs(2)],
        out_specs=tuple(vspecs(2)),
        scratch_shapes=[
            VMEM((ROWS + 2 * EDGE, WIDE), BF16),
            VMEM((WIDE, CH), BF16),
            VMEM((WIDE, PC), BF16),
            VMEM((3, SEG * PITCH, 128), F32),
            VMEM((ROWS + 2 * EDGE * SEG, PC), F32),
            VMEM((ROWS, PC), BF16),
            DMA((3,)),
        ],
        compiler_params=params(16),
        cost_estimate=cost(8 * 528 * WIDE * 384, 8_000_000, 200_000),
        name="pooling",
    )(
        at, *kept(xn, final_switch_matrix, averaging_entry_matrix),
        averaging_cluster_matrices.reshape(PC, PC), averaging_feature_factor.reshape(1, PC),
    )

    mix_send, mix_own = pl.pallas_call(
        states_kernel,
        out_shape=(
            jax.ShapeDtypeStruct((256, CH + PC), BF16),
            jax.ShapeDtypeStruct((256, CH + PC), BF16),
        ),
        in_specs=[smem, *vspecs(2), *hspecs(1), *vspecs(2)],
        out_specs=tuple(vspecs(2)),
        scratch_shapes=[
            VMEM((4, ROWS, CH), F32),
            VMEM((ROWS, CH), F32),
            VMEM((ROWS, CH), F32),
            VMEM((3, ROWS, 128), F32),
            DMA((8,)),
        ],
        compiler_params=params(8),
        cost_estimate=cost(1_000_000_000, 4_000_000, 100_000),
        name="states",
    )(at, got, seg, *kept(kd), gate, pool_mix)

    mix_got = to_sibling(mix_send)
    own_part = pl.pallas_call(
        own_output_kernel,
        out_shape=jax.ShapeDtypeStruct((256, WIDE), F32),
        in_specs=[*vspecs(1), *hspecs(2)],
        out_specs=pl.BlockSpec(memory_space=VMEM),
        scratch_shapes=[VMEM((CH, WIDE), BF16), VMEM((PC, WIDE), BF16), DMA((4, 2))],
        compiler_params=params(6),
        cost_estimate=cost(2 * 256 * 384 * WIDE, 2_500_000),
        name="own_output",
    )(mix_own, *kept(recursive_final_matrix, averaging_final_matrix))
    partial = pl.pallas_call(
        output_kernel,
        out_shape=jax.ShapeDtypeStruct((4, STEP, WIDE), BF16),
        in_specs=vspecs(4),
        out_specs=pl.BlockSpec(memory_space=VMEM),
        compiler_params=params(8),
        cost_estimate=cost(2 * 256 * 384 * WIDE, 2_500_000),
        name="output",
    )(own_part, mix_got, sibling_recursive, sibling_averaging)
    moved = exchange(partial)
    return jnp.sum(moved.astype(F32), axis=0).astype(BF16)


def solution(mesh):
    in_specs = (
        P(("sp", "tp"), None),
        P(),
        P(None, "tp"),
        P(None, "tp"),
        P(None, "tp"),
        P(None, "tp"),
        P(None, None, "tp", None, None),
        P(None, "tp"),
        P(None, "sp"),
        P(None, "sp"),
        P("tp", None, None),
        P("tp"),
        P("tp", None),
        P("tp", None),
    )
    out_specs = P(("sp", "tp"), None)


    return jax.shard_map(local, mesh=mesh, in_specs=in_specs, out_specs=out_specs, check_vma=False)
```

```python
import jax
import jax.numpy as jnp
from jax import lax
from jax.experimental import pallas as pl
from jax.experimental.pallas import tpu as pltpu
from jax.sharding import PartitionSpec as P

FADING_FACTOR = 8.0
epsilon = 1e-06

SEG = 8
STEP = 64
ROWS = SEG * STEP
EDGE = 8
WIDE = 2048
CH = 256
PC = 128
F32 = jnp.float32
BF16 = jnp.bfloat16
VMEM = pltpu.VMEM
HBM = pltpu.HBM
DMA = pltpu.SemaphoreType.DMA
PITCH = STEP + 3 * EDGE


def vspecs(n):
    return [pl.BlockSpec(memory_space=VMEM)] * n


def hspecs(n):
    return [pl.BlockSpec(memory_space=HBM)] * n


def kept(*arrays):
    return [pltpu.with_memory_space_constraint(array, HBM) for array in arrays]


def params(mebibytes):
    return pltpu.CompilerParams(vmem_limit_bytes=mebibytes * 1024 * 1024)


def cost(flops, nbytes, trans=0):
    return pl.CostEstimate(flops=flops, bytes_accessed=nbytes, transcendentals=trans)


def dot(a, b):
    return jnp.dot(a, b, preferred_element_type=F32)


def normalize(read, write, gain_ref, rows):
    total = jnp.zeros((rows, 128), F32)
    for k in range(WIDE // 128):
        v = read(k * 128).astype(F32)
        total = total + v * v
    inv = lax.rsqrt(jnp.sum(total, axis=1, keepdims=True) * (1.0 / WIDE) + epsilon)
    for k in range(WIDE // 128):
        v = read(k * 128).astype(F32)
        gain = gain_ref[0:1, k * 128 : (k + 1) * 128].astype(F32)
        write(k * 128, ((v * inv) * gain).astype(BF16))


def normalize_shard(x_ref, gain_ref, out_ref, base):
    def read(lane):
        return x_ref[:, lane : lane + 128]

    def write(lane, v):
        out_ref[base : base + x_ref.shape[0], lane : lane + 128] = v

    normalize(read, write, gain_ref, x_ref.shape[0])


def spread_kernel(x_ref, out_ref, held_ref, in_sem, out_sem):
    load = pltpu.make_async_copy(x_ref, held_ref, in_sem)
    load.start()
    load.wait()
    copies = [pltpu.make_async_copy(held_ref, out_ref.at[k], out_sem.at[k]) for k in range(4)]
    for copy in copies:
        copy.start()
    for copy in copies:
        copy.wait()


def tables_kernel(maps_ref, extra_ref, bd_ref, spread_ref):
    bd_ref[...] = jnp.zeros_like(bd_ref)
    blank = jnp.zeros((64, 64), BF16)
    for d in range(2):
        for q in range(2):
            for b in range(4):
                block = maps_ref[d, q, b]
                tile = jnp.concatenate([block, blank] if b % 2 == 0 else [blank, block], axis=1)
                col = (d * 2 + q) * CH + (b // 2) * 128
                bd_ref[b * 64 : b * 64 + 64, col : col + 128] = tile
    for d in range(2):
        for j in range(STEP):
            spread_ref[d, j * SEG : (j + 1) * SEG, :] = jnp.broadcast_to(
                extra_ref[d, :, j : j + 1], (SEG, 128)
            )


def placing(at_ref):
    core = lax.rem(at_ref[1], 2)

    def place(y_ref, k, tile, edges):
        for n in range(8):
            parity = core if n < 4 else 1 - core
            base = pl.multiple_of((2 * (n % 4) + parity) * PITCH + EDGE, 8)
            y_ref[k, pl.ds(base, STEP), :] = tile[n * STEP : (n + 1) * STEP]
        if edges:
            one, two = tile[ROWS : ROWS + EDGE], tile[ROWS + EDGE : ROWS + 2 * EDGE]
            y_ref[k, 0:EDGE, :] = jnp.where(core == 1, one, two)
            end = (SEG - 1) * PITCH + EDGE + STEP
            y_ref[k, end : end + EDGE, :] = jnp.where(core == 1, two, one)
            for s in range(SEG - 1):
                low, high = s * PITCH, (s + 1) * PITCH
                y_ref[k, high : high + EDGE, :] = y_ref[k, low + STEP : low + STEP + EDGE, :]
                y_ref[k, low + EDGE + STEP : low + 2 * EDGE + STEP, :] = y_ref[
                    k, high + EDGE : high + 2 * EDGE, :
                ]

    def take(y_ref, k, j):
        return y_ref[k, pl.ds(j + EDGE, SEG, stride=PITCH), :]

    return place, take


def gates_kernel(
    at_ref, own_ref, other_ref, h1_ref, h2_ref, gain_ref,
    rate_ref, ws_hbm, conv_hbm, bd_hbm, speed_hbm, extra_hbm,
    kd_out, xn_out, seg_out, send_out,
    ws_ref, conv_ref, bd_ref, speed_ref, extra_ref,
    xn_ref, y_ref, f_ref, g_ref, kd_ref, seg_ref, send_ref,
    ws_sem, table_sem, kd_sem, xn_sem, seg_sem, send_sem,
):
    place, take = placing(at_ref)
    ws_load = pltpu.make_async_copy(ws_hbm, ws_ref, ws_sem)
    ws_load.start()
    tables = ((conv_hbm, conv_ref), (bd_hbm, bd_ref), (speed_hbm, speed_ref), (extra_hbm, extra_ref))
    table_loads = [
        pltpu.make_async_copy(source, target, table_sem.at[n])
        for n, (source, target) in enumerate(tables)
    ]
    for load in table_loads:
        load.start()
    for n in range(4):
        normalize_shard(own_ref.at[n], gain_ref, xn_ref, n * STEP)
    for n, ref in enumerate((h1_ref, h2_ref)):
        normalize_shard(ref, gain_ref, xn_ref, ROWS + n * EDGE)
    for n in range(4):
        normalize_shard(other_ref.at[n], gain_ref, xn_ref, (n + 4) * STEP)
    xn_copy = pltpu.make_async_copy(xn_ref, xn_out, xn_sem)
    xn_copy.start()
    ws_load.wait()
    value = dot(xn_ref[...], ws_ref[...]).astype(BF16).astype(F32)
    for k in range(2):
        place(y_ref, k, value[:, k * 128 : (k + 1) * 128], True)
    for load in table_loads:
        load.wait()
    taps = conv_ref[...].astype(F32)

    def conv(i, _):
        rows = pl.ds(pl.multiple_of(i * 64, 64), 64)
        for lt in range(2):
            lanes = slice(lt * 128, lt * 128 + 128)
            near = [take(y_ref, lt, i * 8 + j - 2) for j in range(11)]
            out = []
            for j in range(8):
                value = taps[0:1, lanes] * near[j]
                for k in range(1, 4):
                    value = value + taps[k : k + 1, lanes] * near[j + k]
                out.append(value)
            f_ref[rows, lanes] = jnp.concatenate(out, axis=0).astype(BF16)
        return 0

    lax.fori_loop(0, STEP // 8, conv, 0)
    f = f_ref[...]
    for k in range(4):
        g_ref[:, k * 256 : (k + 1) * 256] = dot(f, bd_ref[:, k * 256 : (k + 1) * 256])

    def chunk(i, carry):
        rows = pl.ds(pl.multiple_of(i * 64, 64), 64)
        out = []
        for lt in range(2):
            hf, lf, hb, pb, lb = carry[lt]
            lanes = slice(lt * 128, lt * 128 + 128)
            wide = f_ref[rows, lanes].astype(F32)
            for d in range(2):
                col = d * 512 + lt * 128
                half = half_rate[d][:, lanes]
                recall = jnp.tanh(0.5 * g_ref[rows, col : col + 128])
                inlet = 0.5 * jnp.tanh(0.5 * g_ref[rows, col + 256 : col + 384]) + 0.5
                log_keep = half * recall + half + extra_ref[d, rows, :]
                keep = jnp.exp(log_keep)
                gap = (1.0 + keep * keep) * jnp.tanh(-log_keep)
                drive = gap * lax.rsqrt(jnp.maximum(gap, 1e-37)) * (inlet * wide)
                kd_ref[2 * d, rows, lanes] = keep
                kd_ref[2 * d + 1, rows, lanes] = drive
                for j in range(8):
                    kj = keep[8 * j : 8 * j + 8]
                    uj = drive[8 * j : 8 * j + 8]
                    lj = log_keep[8 * j : 8 * j + 8]
                    if d == 0:
                        hf = kj * hf + uj
                        lf = lf + lj
                    else:
                        hb = hb + pb * uj
                        pb = pb * kj
                        lb = lb + lj
            out.append((hf, lf, hb, pb, lb))
        return tuple(out)

    half_rate = [
        (-0.5 * FADING_FACTOR) * speed_ref[d : d + 1, 0:1] * rate_ref[d : d + 1, :] for d in range(2)
    ]
    zero = jnp.zeros((SEG, 128), F32)
    one = jnp.ones((SEG, 128), F32)
    totals = tuple((zero, zero, zero, one, zero) for _ in range(2))
    kd_copies = []
    for part in range(4):
        totals = lax.fori_loop(2 * part, 2 * part + 2, chunk, totals)
        rows = slice(part * 128, part * 128 + 128)
        copy = pltpu.make_async_copy(
            kd_ref.at[:, rows, :], kd_out.at[:, rows, :], kd_sem.at[part]
        )
        copy.start()
        kd_copies.append(copy)
    row = lax.broadcasted_iota(jnp.int32, (SEG, 128), 0)
    sends = [jnp.zeros((SEG, 128), F32), jnp.zeros((SEG, 128), F32)]
    for lt in range(2):
        hf, lf, hb, _, lb = totals[lt]
        lanes = slice(lt * 128, lt * 128 + 128)
        for d, (log_total, state) in enumerate(((lf, hf), (lb, hb))):
            factor = jnp.exp(log_total)
            for shift in (1, 2, 4):
                move = shift if d == 0 else SEG - shift
                inside = (row >= shift) if d == 0 else (row < SEG - shift)
                earlier_factor = jnp.where(inside, pltpu.roll(factor, move, 0), 1.0)
                earlier_state = jnp.where(inside, pltpu.roll(state, move, 0), 0.0)
                state = factor * earlier_state + state
                factor = factor * earlier_factor
            move = 1 if d == 0 else SEG - 1
            inside = (row >= 1) if d == 0 else (row < SEG - 1)
            seg_ref[2 * d, :, lanes] = jnp.where(inside, pltpu.roll(factor, move, 0), 1.0)
            seg_ref[2 * d + 1, :, lanes] = jnp.where(inside, pltpu.roll(state, move, 0), 0.0)
            end = SEG - 1 if d == 0 else 0
            whole_log = jnp.sum(log_total, axis=0, keepdims=True)
            whole_state = jnp.sum(jnp.where(row == end, state, 0.0), axis=0, keepdims=True)
            sends[d] = jnp.where(row == lt, whole_log, sends[d])
            sends[d] = jnp.where(row == 2 + lt, whole_state, sends[d])
    seg_copy = pltpu.make_async_copy(seg_ref, seg_out, seg_sem)
    seg_copy.start()
    shape = (1, 4, 128)
    forward, backward = (v[0:4].astype(BF16).reshape(shape) for v in sends)
    place_of = at_ref[0]
    for p in range(send_ref.shape[0]):
        send_ref[p : p + 1] = jnp.where(p > place_of, forward, backward)
    send_copy = pltpu.make_async_copy(send_ref, send_out, send_sem)
    send_copy.start()
    for copy in (xn_copy, seg_copy, *kd_copies, send_copy):
        copy.wait()


def pooling_kernel(
    at_ref, xn_hbm, wg_hbm, wp_hbm, cluster_ref, factor_ref,
    gate_ref, mix_ref,
    xn_ref, wg_ref, wp_ref, y_ref, pool_ref, p_ref, sem,
):
    loads = [
        pltpu.make_async_copy(source, target, sem.at[n])
        for n, (source, target) in enumerate(((xn_hbm, xn_ref), (wp_hbm, wp_ref), (wg_hbm, wg_ref)))
    ]
    for load in loads:
        load.start()
    place, take = placing(at_ref)
    position_of, column = at_ref[0], at_ref[1]
    total = at_ref[2]
    code = lax.rem(column, 4)
    loads[0].wait()
    loads[1].wait()
    xn = xn_ref[...]
    place(y_ref, 2, dot(xn, wp_ref[...]).astype(BF16).astype(F32), True)
    loads[2].wait()
    value = dot(xn, wg_ref[...]).astype(BF16).astype(F32)
    for k in range(2):
        place(y_ref, k, value[:, k * 128 : (k + 1) * 128], False)

    def gates(i, _):
        rows = pl.ds(pl.multiple_of(i * 64, 64), 64)
        for lt in range(2):
            tiles = [take(y_ref, lt, i * 8 + j) for j in range(8)]
            gate_ref[rows, lt * 128 : lt * 128 + 128] = jnp.concatenate(tiles, axis=0).astype(BF16)
        return 0

    lax.fori_loop(0, STEP // 8, gates, 0)

    def pools(i, _):
        rows = pl.ds(pl.multiple_of(i * 64, 64), 64)
        tiles = [take(y_ref, 2, i * 8 + j - EDGE) for j in range(8)]
        pool_ref[rows, :] = jnp.concatenate(tiles, axis=0)
        return 0

    lax.fori_loop(0, (STEP + 2 * EDGE) // 8, pools, 0)

    def windows(i, _):
        base = pl.multiple_of(i * 64, 64)
        level = pool_ref[pl.ds(base, 64 + 2 * EDGE * SEG), :]
        centre = level[EDGE * SEG : EDGE * SEG + 64]
        chosen = jnp.zeros((64, PC), F32)
        for k in range(4):
            shift = SEG << k
            size = level.shape[0] - shift
            level = level[:size] + level[shift:]
            begin = (EDGE - (1 << k)) * SEG
            chosen = jnp.where(code == k, level[begin : begin + 64], chosen)
        row = base + lax.broadcasted_iota(jnp.int32, (64, PC), 0)
        position = position_of * ROWS + (row & 7) * STEP + (row >> 3)
        reach = jnp.left_shift(1, code)
        count = jnp.minimum(position + reach, total) - jnp.maximum(position - reach, 0)
        p_ref[pl.ds(base, 64), :] = (chosen / count.astype(F32) - centre).astype(BF16)
        return 0

    lax.fori_loop(0, ROWS // 64, windows, 0)
    grouped = dot(p_ref[...], cluster_ref[...])
    mix_ref[...] = (grouped * factor_ref[...].astype(F32)).astype(BF16)


def states_kernel(
    at_ref, got_ref, seg_ref, kd_hbm, gate_ref, pool_mix_ref,
    send_ref, own_ref,
    kd_ref, hf_ref, hb_ref, mix_ref, kd_sem,
):
    loads = []
    for part in range(4):
        for n, at in enumerate((part, 3 - part)):
            there = (slice(2 * n, 2 * n + 2), slice(at * 128, at * 128 + 128), slice(None))
            loads.append(
                pltpu.make_async_copy(kd_hbm.at[there], kd_ref.at[there], kd_sem.at[2 * part + n])
            )
            loads[-1].start()
    place = at_ref[0]
    core = lax.rem(at_ref[1], 2)
    blocks = got_ref.shape[0]

    def arriving(i, carry):
        ahead, behind = carry
        for k in range(2):
            p = i * 2 + k
            v = got_ref[p].astype(F32)
            ahead = jnp.where(p < place, jnp.exp(v[0:2]) * ahead + v[2:4], ahead)
            p = blocks - 1 - p
            v = got_ref[p].astype(F32)
            behind = jnp.where(p > place, jnp.exp(v[0:2]) * behind + v[2:4], behind)
        return ahead, behind

    zero = jnp.zeros((2, 128), F32)
    carry = lax.fori_loop(0, blocks // 2, arriving, (zero, zero), unroll=min(8, blocks // 2))
    begin = []
    for lt in range(2):
        lanes = slice(lt * 128, lt * 128 + 128)
        for d in range(2):
            begin.append(
                seg_ref[2 * d, :, lanes] * carry[d][lt : lt + 1] + seg_ref[2 * d + 1, :, lanes]
            )

    def walk(i, carry):
        hf0, hb0, hf1, hb1 = carry
        for k in range(8):
            f = pl.ds(pl.multiple_of((i * 8 + k) * SEG, SEG), SEG)
            b = pl.ds(pl.multiple_of((STEP - 1 - i * 8 - k) * SEG, SEG), SEG)
            hf0 = kd_ref[0, f, 0:128] * hf0 + kd_ref[1, f, 0:128]
            hf1 = kd_ref[0, f, 128:256] * hf1 + kd_ref[1, f, 128:256]
            hb0 = kd_ref[2, b, 0:128] * hb0 + kd_ref[3, b, 0:128]
            hb1 = kd_ref[2, b, 128:256] * hb1 + kd_ref[3, b, 128:256]
            hf_ref[f, 0:128] = hf0
            hf_ref[f, 128:256] = hf1
            hb_ref[b, 0:128] = hb0
            hb_ref[b, 128:256] = hb1
        return hf0, hb0, hf1, hb1

    states = tuple(begin)
    for part in range(4):
        loads[2 * part].wait()
        loads[2 * part + 1].wait()
        states = lax.fori_loop(2 * part, 2 * part + 2, walk, states)

    def mixing(i, _):
        rows = pl.ds(pl.multiple_of(i * 64, 64), 64)
        for lt in range(2):
            lanes = slice(lt * 128, lt * 128 + 128)
            v = gate_ref[rows, lanes].astype(F32)
            inner = 0.7978845608028654 * (v + 0.044715 * (v * v * v))
            act = v * (0.5 * (1.0 + jnp.tanh(inner)))
            mix_ref[lt, rows, :] = act * (hf_ref[rows, lanes] + hb_ref[rows, lanes])
        mix_ref[2, rows, :] = pool_mix_ref[rows, :].astype(F32)
        return 0

    lax.fori_loop(0, ROWS // 64, mixing, 0)
    for x in range(4):
        rows = slice(x * STEP, (x + 1) * STEP)
        for k in range(3):
            lanes = slice(k * 128, k * 128 + 128)
            there = mix_ref[k, pl.ds(2 * x + 1 - core, STEP, stride=SEG), :]
            send_ref[rows, lanes] = there.astype(BF16)
            here = mix_ref[k, pl.ds(2 * x + core, STEP, stride=SEG), :]
            own_ref[rows, lanes] = here.astype(BF16)


def weights_in_parts(pairs, sem):
    waits = []
    for k in range(4):
        lanes = slice(k * 512, k * 512 + 512)
        copies = [
            pltpu.make_async_copy(source.at[:, lanes], target.at[:, lanes], sem.at[k, n])
            for n, (source, target) in enumerate(pairs)
        ]
        for copy in copies:
            copy.start()
        waits.append(copies)
    return waits


def own_output_kernel(own_ref, wr_hbm, wp_hbm, out_ref, wr_ref, wp_ref, sem):
    waits = weights_in_parts(((wr_hbm, wr_ref), (wp_hbm, wp_ref)), sem)
    for k in range(4):
        lanes = slice(k * 512, k * 512 + 512)
        for copy in waits[k]:
            copy.wait()
        out_ref[:, lanes] = dot(own_ref[:, 0:CH], wr_ref[:, lanes]) + dot(
            own_ref[:, CH : CH + PC], wp_ref[:, lanes]
        )


def output_kernel(own_ref, got_ref, vr_ref, vp_ref, out_ref):
    for k in range(4):
        lanes = slice(k * 512, k * 512 + 512)
        value = dot(got_ref[:, 0:CH], vr_ref[:, lanes])
        value = value + dot(got_ref[:, CH : CH + PC], vp_ref[:, lanes])
        value = (value + own_ref[:, lanes]).astype(BF16)
        for x in range(4):
            out_ref[x, :, lanes] = value[x * STEP : (x + 1) * STEP]


def local(
    incoming_activity,
    entry_standardize_factor,
    recursive_entry_matrix,
    final_switch_matrix,
    averaging_entry_matrix,
    percolumn_filter_coefficients,
    switch_tiled_matrices,
    prior_fading_odds,
    speed_factors,
    extra_fading_amounts,
    averaging_cluster_matrices,
    averaging_feature_factor,
    recursive_final_matrix,
    averaging_final_matrix,
):
    blocks = lax.axis_size("sp")
    place = lax.axis_index("sp")
    column = lax.axis_index("tp")
    core = column % 2
    same_core = [[0, 2, 4, 6], [1, 3, 5, 7]]
    sibling = [(k, k ^ 1) for k in range(8)]

    def exchange(v):
        return lax.all_to_all(
            v, "tp", split_axis=0, concat_axis=0, tiled=True, axis_index_groups=same_core
        )

    def edge_pairs(cross):
        pairs = []
        for sp in range(blocks):
            for tp in range(8):
                to = sp + 1 if tp % 2 else sp - 1
                if 0 <= to < blocks:
                    pairs.append((sp * 8 + tp, to * 8 + (tp ^ cross)))
        return pairs

    def to_sibling(v):
        return lax.ppermute(v, "tp", sibling)

    smem = pl.BlockSpec(memory_space=pltpu.SMEM)
    at = jnp.stack([place, column, jnp.asarray(blocks * ROWS)]).astype(jnp.int32)
    spread = pl.pallas_call(
        spread_kernel,
        out_shape=HBM((4, STEP, WIDE), BF16),
        in_specs=hspecs(1),
        out_specs=pl.BlockSpec(memory_space=HBM),
        scratch_shapes=[VMEM((STEP, WIDE), BF16), DMA, DMA((4,))],
        compiler_params=params(2),
        cost_estimate=cost(0, 1_300_000),
        name="spread",
    )(*kept(incoming_activity))
    x_own = exchange(spread)
    sibling_recursive = lax.ppermute(recursive_final_matrix, "tp", sibling)
    sibling_averaging = lax.ppermute(averaging_final_matrix, "tp", sibling)
    x_other = to_sibling(x_own)
    edge = lax.dynamic_slice(
        x_own, (3 * core, (STEP - EDGE) * core, 0), (1, EDGE, WIDE)
    ).reshape(EDGE, WIDE)
    edge_same = lax.ppermute(edge, ("sp", "tp"), edge_pairs(0))
    edge_cross = lax.ppermute(edge, ("sp", "tp"), edge_pairs(1))

    at = jnp.stack([place, column, jnp.asarray(blocks * ROWS)]).astype(jnp.int32)
    gain = entry_standardize_factor.reshape(1, WIDE)
    rate = jax.nn.softplus(-prior_fading_odds)
    maps, extra = pl.pallas_call(
        tables_kernel,
        out_shape=(
            HBM((CH, 4 * CH), BF16),
            HBM((2, ROWS, 128), F32),
        ),
        in_specs=vspecs(2),
        out_specs=tuple(vspecs(2)),
        compiler_params=params(4),
        cost_estimate=cost(1_000_000, 2_000_000),
        name="tables",
    )(switch_tiled_matrices, extra_fading_amounts.reshape(2, SEG, STEP))

    kd, xn, seg, send = pl.pallas_call(
        gates_kernel,
        out_shape=(
            HBM((4, ROWS, CH), F32),
            HBM((ROWS + 2 * EDGE, WIDE), BF16),
            HBM((4, SEG, CH), F32),
            HBM((blocks, 4, 128), BF16),
        ),
        in_specs=[smem, *vspecs(6), *hspecs(5)],
        out_specs=tuple(hspecs(4)),
        scratch_shapes=[
            VMEM((WIDE, CH), BF16),
            VMEM((4, CH), BF16),
            VMEM((CH, 4 * CH), BF16),
            VMEM((2, ROWS), F32),
            VMEM((2, ROWS, 128), F32),
            VMEM((ROWS + 2 * EDGE, WIDE), BF16),
            VMEM((2, (SEG + 1) * PITCH, 128), F32),
            VMEM((ROWS, CH), BF16),
            VMEM((ROWS, 4 * CH), F32),
            VMEM((4, ROWS, CH), F32),
            VMEM((4, SEG, CH), F32),
            VMEM((blocks, 4, 128), BF16),
            DMA,
            DMA((4,)),
            DMA((4,)),
            DMA,
            DMA,
            DMA,
        ],
        compiler_params=params(20),
        cost_estimate=cost(2 * 528 * WIDE * 256, 8_000_000, 1_000_000),
        name="gates",
    )(
        at, x_own, x_other, edge_same, edge_cross, gain, rate,
        *kept(recursive_entry_matrix, percolumn_filter_coefficients, maps, speed_factors, extra),
    )

    got = lax.all_to_all(send, "sp", split_axis=0, concat_axis=0, tiled=True)

    gate, pool_mix = pl.pallas_call(
        pooling_kernel,
        out_shape=(
            jax.ShapeDtypeStruct((ROWS, CH), BF16),
            jax.ShapeDtypeStruct((ROWS, PC), BF16),
        ),
        in_specs=[smem, *hspecs(3), *vspecs(2)],
        out_specs=tuple(vspecs(2)),
        scratch_shapes=[
            VMEM((ROWS + 2 * EDGE, WIDE), BF16),
            VMEM((WIDE, CH), BF16),
            VMEM((WIDE, PC), BF16),
            VMEM((3, (SEG + 1) * PITCH, 128), F32),
            VMEM((ROWS + 2 * EDGE * SEG, PC), F32),
            VMEM((ROWS, PC), BF16),
            DMA((3,)),
        ],
        compiler_params=params(16),
        cost_estimate=cost(8 * 528 * WIDE * 384, 8_000_000, 200_000),
        name="pooling",
    )(
        at, *kept(xn, final_switch_matrix, averaging_entry_matrix),
        averaging_cluster_matrices.reshape(PC, PC), averaging_feature_factor.reshape(1, PC),
    )

    mix_send, mix_own = pl.pallas_call(
        states_kernel,
        out_shape=(
            jax.ShapeDtypeStruct((256, CH + PC), BF16),
            jax.ShapeDtypeStruct((256, CH + PC), BF16),
        ),
        in_specs=[smem, *vspecs(2), *hspecs(1), *vspecs(2)],
        out_specs=tuple(vspecs(2)),
        scratch_shapes=[
            VMEM((4, ROWS, CH), F32),
            VMEM((ROWS, CH), F32),
            VMEM((ROWS, CH), F32),
            VMEM((3, ROWS + SEG, 128), F32),
            DMA((8,)),
        ],
        compiler_params=params(8),
        cost_estimate=cost(1_000_000_000, 4_000_000, 100_000),
        name="states",
    )(at, got, seg, *kept(kd), gate, pool_mix)

    mix_got = to_sibling(mix_send)
    own_part = pl.pallas_call(
        own_output_kernel,
        out_shape=jax.ShapeDtypeStruct((256, WIDE), F32),
        in_specs=[*vspecs(1), *hspecs(2)],
        out_specs=pl.BlockSpec(memory_space=VMEM),
        scratch_shapes=[VMEM((CH, WIDE), BF16), VMEM((PC, WIDE), BF16), DMA((4, 2))],
        compiler_params=params(6),
        cost_estimate=cost(2 * 256 * 384 * WIDE, 2_500_000),
        name="own_output",
    )(mix_own, *kept(recursive_final_matrix, averaging_final_matrix))
    partial = pl.pallas_call(
        output_kernel,
        out_shape=jax.ShapeDtypeStruct((4, STEP, WIDE), BF16),
        in_specs=vspecs(4),
        out_specs=pl.BlockSpec(memory_space=VMEM),
        compiler_params=params(8),
        cost_estimate=cost(2 * 256 * 384 * WIDE, 2_500_000),
        name="output",
    )(own_part, mix_got, sibling_recursive, sibling_averaging)
    moved = exchange(partial)
    return jnp.sum(moved.astype(F32), axis=0).astype(BF16)


def solution(mesh):
    in_specs = (
        P(("sp", "tp"), None),
        P(),
        P(None, "tp"),
        P(None, "tp"),
        P(None, "tp"),
        P(None, "tp"),
        P(None, None, "tp", None, None),
        P(None, "tp"),
        P(None, "sp"),
        P(None, "sp"),
        P("tp", None, None),
        P("tp"),
        P("tp", None),
        P("tp", None),
    )
    out_specs = P(("sp", "tp"), None)


    return jax.shard_map(local, mesh=mesh, in_specs=in_specs, out_specs=out_specs, check_vma=False)
```
